256 devices in a mesh: ep: 64 (over z, x, core), tp: 4 (over y).
Axes of the slice: x: 4, y: 4, z: 8, core: 2. Of those that a mesh axis runs over, the one named last changes fastest.
Arguments:
- tokens: bfloat16 [1536, 4096], P('ep'), may hold values from -6 to 6
- norm_gain: bfloat16 [4096], replicated, may hold values from 0.099609375 to 1.8984375
- w_query: bfloat16 [4096, 1024], P('ep', 'tp'), may hold values from -0.09375 to 0.09375
- w_key: bfloat16 [4096, 1024], P('ep', 'tp'), may hold values from -0.09375 to 0.09375
- w_value: bfloat16 [4096, 2048], P('ep', 'tp'), may hold values from -0.09375 to 0.09375
- w_rgate: bfloat16 [4096, 2048], P('ep', 'tp'), may hold values from -0.09375 to 0.09375
- w_decay: bfloat16 [4096, 1024], P('ep', 'tp'), may hold values from -0.375 to 0.375
- decay_shift: float32 [1536, 1024], P('ep', 'tp'), may hold values from -2 to 0
- state: float32 [1536, 8, 128, 256], P('ep', 'tp'), may hold values from -6 to 6
- head_gain: bfloat16 [2048], P('tp'), may hold values from 0.099609375 to 1.8984375
- w_out: bfloat16 [2048, 4096], P('tp', 'ep'), may hold values from -0.125 to 0.125
- ffn_gain: bfloat16 [4096], replicated, may hold values from 0.099609375 to 1.8984375
- w_gate: bfloat16 [64, 4096, 1024], P('ep', None, 'tp'), may hold values from -0.21875 to 0.21875
- w_lin: bfloat16 [64, 4096, 1024], P('ep', None, 'tp'), may hold values from -0.21875 to 0.21875
- w_down: bfloat16 [64, 1024, 4096], P('ep', 'tp'), may hold values from -0.046875 to 0.046875
- expert_ids: int32 [1536, 4], P('ep'), may hold values from 0 to 63, all different within a row; in each aligned block of 24 rows (0 to 23, 24 to 47, ...) at most 3 rows name the same one
- route_weight: float32 [1536, 4], P('ep'), may hold values from 0.2 to 1
Outputs:
- result: bfloat16 [1536, 4096], P('ep')
The draws below stay inside these ranges and needn't reach their ends.
Inputs may be any that keep to these rules, and one draw needn't show every extreme that they name: `expert_ids`: each row names 4 different experts; among the rows of one index of ep no expert is named more than 3 times, a bound that some block reaches.
All inputs are finite; a program needn't handle non-finite values.
Results may differ from the reference program's by a relative error of at most 0.022.
Values may be sent and summed in bfloat16 or wider, within the bound.
No kernel may reach another device: no remote copies, remote signals or barrier semaphores. Data moves between devices by JAX's collectives and lax.ppermute only.
A program may use at most 128 MiB of HBM per device.

```python
import math
import jax
import jax.numpy as jnp
import numpy as np
from jax import lax

D = 4096
HEADS = 8
HK = 128
HV = 256
DK = 1024
DV = 2048
DE = 1024
TOP_K = 4
EXPERTS = 64
SEQ_DEV = 24
SEQS = 1536
CAP = 3
N_EP = 64
N_TP = 4


def steps_of(stream_key, shape, shards, smallest, largest):
    def one(axis_at, shards_of):
        steps = jax.random.uniform(jax.random.fold_in(jax.random.fold_in(stream_key, 6), axis_at), (shards_of,), jnp.float32, smallest / len(shards), largest / len(shards))
        return jnp.repeat(jnp.exp(steps), shape[axis_at] // shards_of).reshape((-1,) + (1,) * (len(shape) - axis_at - 1))

    level = one(*shards[0])
    for cut in shards[1:]:
        level = level * one(*cut)
    return level


def routed_block(key, own, number, rows, number_of, top, reach, skew):
    ranking = jax.random.permutation(key, number_of)
    crowded, usual = load_shares(number_of, rows * top, reach, skew, True), load_shares(number_of, rows * top, reach, skew, False)
    places = jnp.arange(number_of)

    def named(lengths, offset_by):
        used = int((lengths > 0).sum())
        fixed = max(1, used // 4)
        moved = fixed + (places - fixed + offset_by * (used - fixed)) % max(1, number_of - fixed)
        return jnp.zeros((number_of,), jnp.int32).at[ranking[jnp.where(places < fixed, places, moved)]].set(jnp.asarray(lengths, jnp.int32))

    lengths = jnp.where(number % 4 == 0, named(crowded, number // 4), named(usual, number - number // 4 - 1))
    mixed = jax.random.permutation(jax.random.fold_in(own, 3), number_of)
    giver, receiver = mixed[0:number_of // 2 * 2:2], mixed[1:number_of // 2 * 2:2]
    room = jnp.minimum(lengths[giver] - 1, reach - lengths[receiver]) // 2
    room = jnp.where((giver == ranking[0]) | (receiver == ranking[0]) | (lengths[receiver] == 0), 0, jnp.maximum(room, 0))
    moved = jax.random.randint(jax.random.fold_in(own, 4), (number_of // 2,), 0, 1 << 20) % (room + 1)
    lengths = lengths.at[giver].add(-moved).at[receiver].add(moved)
    labels = jnp.searchsorted(jnp.cumsum(lengths), jnp.arange(rows * top), side="right").astype(jnp.int32)
    table = labels.reshape(top, rows).T
    table = table[jax.random.permutation(jax.random.fold_in(own, 1), rows)]
    offset_by = jax.random.randint(jax.random.fold_in(own, 2), (rows, 1), 0, top)
    return jnp.take_along_axis(table, (jnp.arange(top)[None, :] + offset_by) % top, axis=1)


def load_shares(count, total, most, slope, full):
    loads = [(1 << 20) // math.isqrt(standing ** slope) + 1 for standing in range(1, count + 1)]
    largest = most if full else min(most, max(-(-total // count), total * loads[0] // sum(loads)))
    least = 1 if total - largest >= count - 1 else 0
    given, rest = [largest] + [least] * (count - 1), total - largest - least * (count - 1)
    while rest > 0:
        candidates = [i for i in range(1, count) if given[i] < largest] or [i for i in range(1, count) if given[i] < most]
        pool, left = sum([loads[i] for i in candidates]), rest
        for i in candidates:
            addition = min(most - given[i], max(1, left * loads[i] // pool), rest)
            given[i] = given[i] + addition
            rest = rest - addition
    return np.array(given)


def centred(own_key, shape, deviation, most, shards=(), held_as=jnp.bfloat16):
    factor_of = steps_of(own_key, shape, shards, -0.22, 0.18) if shards else 1.0
    result = jax.random.normal(own_key, shape, jnp.float32) * deviation * factor_of
    return jnp.minimum(jnp.maximum(result, -most), most).astype(held_as)


def setup_inputs(seed: int = 0) -> dict:
    seeds = jax.random.split(jax.random.key(seed), 18)
    tokens = centred(seeds[0], (SEQS, D), 1.0, 6.0, ((0, 64),))
    norm_gain = jnp.clip(1.0 + 0.18 * jax.random.normal(seeds[1], (D,), jnp.float32), 0.099609375, 1.8984375).astype(jnp.bfloat16)
    w_query = centred(seeds[2], (D, DK), D ** -0.5, 0.09375, ((0, 64), (1, 4)))
    w_key = centred(seeds[3], (D, DK), D ** -0.5, 0.09375, ((0, 64), (1, 4)))
    w_value = centred(seeds[4], (D, DV), D ** -0.5, 0.09375, ((0, 64), (1, 4)))
    w_rgate = centred(seeds[5], (D, DV), D ** -0.5, 0.09375, ((0, 64), (1, 4)))
    w_decay = centred(seeds[6], (D, DK), (D // 16) ** -0.5, 0.375, ((0, 64), (1, 4)))
    decay_shift = jnp.clip(-2.0 + 2.0 * jax.random.uniform(seeds[7], (SEQS, DK), jnp.float32) ** steps_of(seeds[7], (SEQS, DK), ((0, 64), (1, 4)), -0.2, 0.2), -2.0, 0.0)
    state = centred(seeds[8], (SEQS, HEADS, HK, HV), 1.0, 6.0, ((0, 64), (1, 4)), jnp.float32)
    head_gain = jnp.clip(1.0 + 0.18 * jax.random.normal(seeds[9], (DV,), jnp.float32), 0.099609375, 1.8984375).astype(jnp.bfloat16)
    w_out = centred(seeds[10], (DV, D), DV ** -0.5, 0.125, ((0, 4), (1, 64)))
    ffn_gain = jnp.clip(1.0 + 0.18 * jax.random.normal(seeds[11], (D,), jnp.float32), 0.099609375, 1.8984375).astype(jnp.bfloat16)
    w_gate = centred(seeds[12], (EXPERTS, D, DE), (D // 6) ** -0.5, 0.21875, ((0, 64), (2, 4)))
    w_lin = centred(seeds[13], (EXPERTS, D, DE), (D // 6) ** -0.5, 0.21875, ((0, 64), (2, 4)))
    w_down = centred(seeds[14], (EXPERTS, DE, D), (DE * 16) ** -0.5, 0.046875, ((0, 64), (1, 4)))
    expert_ids_keys = jax.random.split(jax.random.fold_in(seeds[15], 1), SEQS // SEQ_DEV)
    expert_ids_turns = jax.random.permutation(jax.random.fold_in(seeds[15], 3), SEQS // SEQ_DEV)
    expert_ids = jax.vmap(lambda own, number: routed_block(jax.random.fold_in(seeds[15], 2), own, number, SEQ_DEV, EXPERTS, TOP_K, CAP, 2))(expert_ids_keys, expert_ids_turns).reshape((SEQS, TOP_K))
    route_weight = jnp.clip(0.2 + 0.8 * jax.random.uniform(seeds[16], (SEQS, TOP_K), jnp.float32) ** steps_of(seeds[16], (SEQS, TOP_K), ((0, 64),), -0.2, 0.2), 0.2, 1.0)
    return {"tokens": tokens, "norm_gain": norm_gain, "w_query": w_query, "w_key": w_key, "w_value": w_value, "w_rgate": w_rgate, "w_decay": w_decay, "decay_shift": decay_shift, "state": state, "head_gain": head_gain, "w_out": w_out, "ffn_gain": ffn_gain, "w_gate": w_gate, "w_lin": w_lin, "w_down": w_down, "expert_ids": expert_ids, "route_weight": route_weight}


eps = 1e-06
tau = 16.0
limit = 7.0
glu_alpha = 1.702

def rms_scale(values, gain):
    meansq = lax.optimization_barrier(jnp.mean(values * values, axis=-1, keepdims=True))
    return values * lax.rsqrt(meansq + eps) * gain

def expert_apply(rows, gate_w, lin_w, down_w):
    gate = jnp.dot(rows, gate_w, preferred_element_type=jnp.float32)
    linear = jnp.dot(rows, lin_w, preferred_element_type=jnp.float32)
    gate = jnp.minimum(gate, limit)
    linear = jnp.clip(linear, -limit, limit)
    act = (gate * jax.nn.sigmoid(glu_alpha * gate) * (linear + 1.0)).astype(jnp.bfloat16)
    span = act.shape[1] // N_TP
    total = jnp.zeros((rows.shape[0], down_w.shape[1]), jnp.float32)
    for portion in range(N_TP):
        piece = jnp.dot(act[:, portion * span:(portion + 1) * span], down_w[portion * span:(portion + 1) * span], preferred_element_type=jnp.float32)
        total = total + lax.optimization_barrier(piece.astype(jnp.bfloat16)).astype(jnp.float32)
    return total.astype(jnp.bfloat16)

def reference(tokens, norm_gain, w_query, w_key, w_value, w_rgate, w_decay, decay_shift, state, head_gain, w_out, ffn_gain, w_gate, w_lin, w_down, expert_ids, route_weight):
    seqs = tokens.shape[0]
    width = tokens.shape[1]
    heads = state.shape[1]
    key_dim = state.shape[2]
    val_dim = state.shape[3]
    inputs = tokens.astype(jnp.float32)
    normed = rms_scale(inputs, norm_gain.astype(jnp.float32)).astype(jnp.bfloat16)
    queries = jnp.dot(normed, w_query, preferred_element_type=jnp.float32).astype(jnp.bfloat16)
    keys_new = jnp.dot(normed, w_key, preferred_element_type=jnp.float32).astype(jnp.bfloat16)
    values_new = jnp.dot(normed, w_value, preferred_element_type=jnp.float32).astype(jnp.bfloat16)
    rgates = jnp.dot(normed, w_rgate, preferred_element_type=jnp.float32).astype(jnp.bfloat16)
    decay_pre = jnp.dot(normed, w_decay, preferred_element_type=jnp.float32).astype(jnp.bfloat16)
    log_decay = jax.nn.log_sigmoid(decay_pre.astype(jnp.float32)) / tau + decay_shift
    q_rows = queries.astype(jnp.float32).reshape(seqs, heads, key_dim) * key_dim ** (-0.5)
    k_rows = keys_new.astype(jnp.float32).reshape(seqs, heads, key_dim)
    v_rows = values_new.astype(jnp.float32).reshape(seqs, heads, val_dim)
    new_state = jnp.exp(log_decay.reshape(seqs, heads, key_dim))[..., None] * state + k_rows[..., None] * v_rows[:, :, None, :]
    read = jnp.einsum('shk,shkv->shv', q_rows, new_state, precision=lax.Precision.HIGHEST)
    gated = rms_scale(read, head_gain.astype(jnp.float32).reshape(heads, val_dim))
    gated = gated * jax.nn.silu(rgates.astype(jnp.float32).reshape(seqs, heads, val_dim))
    gated = gated.reshape(seqs, heads * val_dim).astype(jnp.bfloat16)
    span = heads * val_dim // N_TP
    mixed = jnp.zeros((seqs, width), jnp.float32)
    for portion in range(N_TP):
        piece = jnp.dot(gated[:, portion * span:(portion + 1) * span], w_out[portion * span:(portion + 1) * span], preferred_element_type=jnp.float32)
        mixed = mixed + lax.optimization_barrier(piece.astype(jnp.bfloat16)).astype(jnp.float32)
    mixed = mixed.astype(jnp.bfloat16)
    stream = inputs + mixed.astype(jnp.float32)
    ffn_in = rms_scale(stream, ffn_gain.astype(jnp.float32)).astype(jnp.bfloat16)
    experts = w_gate.shape[0]
    top = expert_ids.shape[1]
    slots = N_EP * CAP
    flat_ids = expert_ids.reshape(-1).astype(jnp.int32)
    onehot = (flat_ids[:, None] == jnp.arange(experts, dtype=jnp.int32)[None, :]).astype(jnp.int32)
    rank = lax.optimization_barrier(jnp.sum((jnp.cumsum(onehot, axis=0) - onehot) * onehot, axis=1)).astype(jnp.int32)
    dest = (flat_ids * slots + rank).astype(jnp.int32)
    owner = jnp.repeat(jnp.arange(seqs, dtype=jnp.int32), top)
    table = jnp.full((experts * slots,), seqs, jnp.int32).at[dest].set(owner)
    padded = jnp.concatenate([ffn_in, jnp.zeros((1, width), jnp.bfloat16)], axis=0)

    def one_expert(index):
        picks = lax.dynamic_slice_in_dim(table, (index * slots).astype(jnp.int32), slots)
        return expert_apply(padded[picks], w_gate[index], w_lin[index], w_down[index])
    outputs = lax.map(one_expert, jnp.arange(experts, dtype=jnp.int32))
    picked = outputs.reshape(experts * slots, width)[dest].astype(jnp.float32).reshape(seqs, top, width)
    routed = lax.optimization_barrier(jnp.sum(picked * route_weight[..., None], axis=1))
    return (stream + routed).astype(jnp.bfloat16)
```

```python
import functools
import jax
import jax.numpy as jnp
from jax import lax
from jax.experimental import pallas as pl
from jax.experimental.pallas import tpu as pltpu
from jax.sharding import Mesh
from jax.sharding import PartitionSpec as P


EP = ("ep_0", "ep_1", "ep_2")
Z, X, C, T = "ep_0", "ep_1", "ep_2", "tp"

eps = 1e-06
tau = 16.0
limit = 7.0
glu_alpha = 1.702
CAP = 3

f32 = jnp.float32
bf16 = jnp.bfloat16


def shift(value, axis, by):
    n = lax.axis_size(axis)
    return lax.ppermute(value, axis, [(i, (i + by) % n) for i in range(n)])


def order_of(n):
    return sorted(range(1, n), key=lambda s: (-min(s, n - s), s))


def pack_kernel(*refs):
    out, at = refs[-1], 0
    for ref in refs[:-1]:
        out[:, at : at + ref.shape[1]] = ref[...]
        at += ref.shape[1]


def pack(arrays):
    rows = arrays[0].shape[0]
    cols = sum(a.shape[1] for a in arrays)
    return pl.pallas_call(
        pack_kernel,
        out_shape=jax.ShapeDtypeStruct((rows, cols), arrays[0].dtype),
        cost_estimate=pl.CostEstimate(
            flops=1000, bytes_accessed=4 * rows * cols, transcendentals=0
        ),
        name="pack",
    )(*arrays)


def project_kernel(nz, nx, where, tok, *refs):
    own, other = refs[:nx], refs[nx : 2 * nx]
    outs = refs[2 * nx : 2 * nx + nz]
    weight = refs[-1]
    z, x, c = where[0], where[1], where[2]
    rows = own[0].shape[0]
    for i in range(nx):
        base = lax.rem(x - i + nx, nx) * (2 * rows)
        weight[pl.ds(pl.multiple_of(base + c * rows, rows), rows), :] = own[i][...]
        weight[pl.ds(pl.multiple_of(base + (1 - c) * rows, rows), rows), :] = other[i][...]
    seqs = outs[0].shape[0]
    total = jnp.dot(
        tok[...].reshape(nz * seqs, tok.shape[2]), weight[...], preferred_element_type=f32
    ).astype(bf16)
    for i in range(nz):
        outs[i][...] = total[i * seqs : (i + 1) * seqs, :]


def project(where, tok, own, other):
    nz, seqs, depth = tok.shape
    nx, cols = len(own), own[0].shape[1]
    return pl.pallas_call(
        functools.partial(project_kernel, nz, nx),
        out_shape=[jax.ShapeDtypeStruct((seqs, cols), bf16)] * nz,
        in_specs=[pl.BlockSpec(memory_space=pltpu.SMEM)]
        + [pl.BlockSpec(memory_space=pltpu.VMEM)] * (1 + 2 * nx),
        out_specs=[pl.BlockSpec(memory_space=pltpu.VMEM)] * nz,
        scratch_shapes=[pltpu.VMEM((depth, cols), bf16)],
        cost_estimate=pl.CostEstimate(
            flops=2 * nz * seqs * depth * cols,
            bytes_accessed=2 * depth * cols,
            transcendentals=0,
        ),
        name="project",
    )(where, tok, *own, *other)


def on_device(
    tokens,
    norm_gain,
    w_query,
    w_key,
    w_value,
    w_rgate,
    w_decay,
    decay_shift,
    state,
    head_gain,
    w_out,
    ffn_gain,
    w_gate,
    w_lin,
    w_down,
    expert_ids,
    route_weight,
):
    seq_dev, width = tokens.shape
    heads_dev, key_dim, val_dim = state.shape[1:]
    key_cols = w_query.shape[1]
    val_cols = w_value.shape[1]
    nz, nx, nt = lax.axis_size(Z), lax.axis_size(X), lax.axis_size(T)
    n_ep = lax.axis_size(EP)
    z, x, c, t = (lax.axis_index(a) for a in (Z, X, C, T))
    where = jnp.stack([z, x, c, t]).astype(jnp.int32)
    rows_dev = w_query.shape[0]
    z_cols = width // nz
    part = width // nt

    packed = pack((w_query, w_key, w_decay, w_value, w_rgate))
    own = [packed] + [shift(packed, X, i) for i in range(1, nx)]
    other = [shift(w, C, 1) for w in own]

    inputs = tokens.astype(f32)
    scaled = (inputs * norm_gain.astype(f32)).astype(bf16)
    tok_parts = jnp.moveaxis(scaled.reshape(seq_dev, nz, z_cols), 1, 0)
    out_t = w_out.T
    depth_out = out_t.shape[1]
    out_part = jnp.broadcast_to(
        jnp.moveaxis(out_t.reshape(rows_dev, depth_out // z_cols, z_cols), 1, 0).reshape(
            1, -1, z_cols
        ),
        (nz, rows_dev * depth_out // z_cols, z_cols),
    )
    moved = lax.all_to_all(
        jnp.concatenate([tok_parts, out_part], axis=1), Z, 0, 0, tiled=True
    )
    tok = moved[:, :seq_dev]
    out_z = moved[:, seq_dev:].reshape(nz * rows_dev, depth_out)

    down = w_down[0]
    own_down = lax.dynamic_slice_in_dim(down, t * part, part, 1)
    downs = [own_down] + [
        shift(lax.dynamic_slice_in_dim(down, lax.rem(t + s, nt) * part, part, 1), T, s)
        for s in range(1, nt)
    ]

    parts = project(where, tok, own, other)
    stacked = jnp.stack(parts)
    arrived = [lax.dynamic_index_in_dim(stacked, z, 0, False)]
    for s in order_of(nz):
        block = lax.dynamic_index_in_dim(stacked, lax.rem(z + s, nz), 0, False)
        arrived.append(shift(block, Z, s))

    out_x = [out_z] + [shift(out_z, X, i) for i in range(1, nx)]
    out_own = jnp.stack(out_x)
    out_other = shift(out_own, C, 1)

    first_scale = lax.rsqrt(jnp.mean(inputs * inputs, axis=-1, keepdims=True) + eps)
    projected = functools.reduce(jnp.add, [a.astype(f32) for a in arrived]) * first_scale
    q_rows = projected[:, :key_cols].reshape(seq_dev, heads_dev, key_dim) * key_dim ** (-0.5)
    k_rows = projected[:, key_cols : 2 * key_cols].reshape(seq_dev, heads_dev, key_dim)
    decay_pre = projected[:, 2 * key_cols : 3 * key_cols]
    v_rows = projected[:, 3 * key_cols : 3 * key_cols + val_cols].reshape(
        seq_dev, heads_dev, val_dim
    )
    rgates = projected[:, 3 * key_cols + val_cols :].reshape(seq_dev, heads_dev, val_dim)
    log_decay = jax.nn.log_sigmoid(decay_pre) / tau + decay_shift
    new_state = (
        jnp.exp(log_decay.reshape(seq_dev, heads_dev, key_dim))[..., None] * state
        + k_rows[..., None] * v_rows[:, :, None, :]
    )
    read = jnp.einsum("shk,shkv->shv", q_rows, new_state)
    read_sq = jnp.mean(read * read, axis=-1, keepdims=True)
    gated = (
        read
        * lax.rsqrt(read_sq + eps)
        * head_gain.astype(f32).reshape(heads_dev, val_dim)
        * jax.nn.silu(rgates)
    )
    gated = gated.reshape(seq_dev, heads_dev * val_dim).astype(bf16)

    mixed_own = jnp.einsum("sk,xnk->xsn", gated, out_own, preferred_element_type=f32)
    mixed_other = jnp.einsum("sk,xnk->xsn", gated, out_other, preferred_element_type=f32)
    by_core = jnp.where(
        c == 0,
        jnp.stack([mixed_own, mixed_other]),
        jnp.stack([mixed_other, mixed_own]),
    ).astype(bf16)
    turned = jnp.stack(
        [lax.dynamic_index_in_dim(by_core, lax.rem(x - i + nx, nx), 1, False) for i in range(nx)], 1
    )
    full = turned.reshape(2, nx, seq_dev, nz, rows_dev)
    full = jnp.transpose(full, (2, 3, 1, 0, 4)).reshape(seq_dev, width)
    mixed_own = lax.dynamic_slice_in_dim(full, t * part, part, 1).astype(f32)
    for s in range(1, nt):
        block = lax.dynamic_slice_in_dim(full, lax.rem(t + s, nt) * part, part, 1)
        mixed_own = mixed_own + shift(block, T, s).astype(f32)
    stream = lax.dynamic_slice_in_dim(inputs, t * part, part, 1) + mixed_own
    gain_of = ffn_gain.astype(f32)
    ffn_part = (stream * lax.dynamic_slice_in_dim(gain_of, t * part, part)).astype(bf16)

    top = expert_ids.shape[1]
    flat_ids = expert_ids.reshape(-1)
    onehot = (flat_ids[:, None] == jnp.arange(n_ep, dtype=jnp.int32)[None, :]).astype(jnp.int32)
    rank = jnp.sum((jnp.cumsum(onehot, axis=0) - onehot) * onehot, axis=1)
    slot_of = (flat_ids * CAP + rank).reshape(seq_dev, top)
    slots = n_ep * CAP
    hits = jnp.arange(slots, dtype=jnp.int32)[None, None, :] == slot_of[:, :, None]
    dispatch = jnp.sum(hits.astype(bf16), axis=1)
    combine = jnp.sum(jnp.where(hits, route_weight[:, :, None], 0.0), axis=1)

    outbound = jnp.einsum("sn,sd->nd", dispatch, ffn_part, preferred_element_type=f32)
    outbound = outbound.astype(bf16).reshape(n_ep, CAP, part)
    rows = lax.all_to_all(outbound, EP, 0, 0, tiled=True).reshape(slots, part)

    gate, lin, sumsq = 0.0, 0.0, 0.0
    for s in range(nt):
        piece = rows if s == 0 else shift(rows, T, s)
        start = lax.rem(t - s + nt, nt) * part
        plain = piece.astype(f32) / lax.dynamic_slice_in_dim(gain_of, start, part)
        sumsq = sumsq + jnp.sum(plain * plain, axis=-1, keepdims=True)
        gate = gate + jnp.dot(
            piece,
            lax.dynamic_slice_in_dim(w_gate[0], start, part, 0),
            preferred_element_type=f32,
        )
        lin = lin + jnp.dot(
            piece,
            lax.dynamic_slice_in_dim(w_lin[0], start, part, 0),
            preferred_element_type=f32,
        )
    scale = lax.rsqrt(sumsq / width + eps)
    gate = jnp.minimum(gate * scale, limit)
    lin = jnp.clip(lin * scale, -limit, limit)
    act = (gate * jax.nn.sigmoid(glu_alpha * gate) * (lin + 1.0)).astype(bf16)
    done = 0.0
    for s in range(nt):
        piece = act if s == 0 else shift(act, T, s)
        done = done + jnp.dot(piece, downs[s], preferred_element_type=f32)
    returned = lax.all_to_all(
        done.astype(bf16).reshape(n_ep, CAP, part), EP, 0, 0, tiled=True
    ).reshape(slots, part)
    routed = jnp.dot(
        combine,
        returned.astype(f32),
        preferred_element_type=f32,
        precision=lax.Precision.HIGHEST,
    )
    result_part = (stream + routed).astype(bf16)
    result = jnp.zeros((seq_dev, width), bf16)
    for s in range(nt):
        piece = result_part if s == 0 else shift(result_part, T, s)
        result = lax.dynamic_update_slice_in_dim(
            result, piece, lax.rem(t - s + nt, nt) * part, 1
        )
    return result


def solution(mesh):
    sizes = dict(mesh.shape)
    torus = Mesh(
        mesh.devices.reshape(sizes.get("z", 8), sizes.get("x", 4), 2, sizes["tp"]),
        (Z, X, C, T),
    )
    return jax.shard_map(
        on_device,
        mesh=torus,
        in_specs=(
            P(EP, None),
            P(),
            P(EP, T),
            P(EP, T),
            P(EP, T),
            P(EP, T),
            P(EP, T),
            P(EP, T),
            P(EP, T, None, None),
            P(T),
            P(T, EP),
            P(),
            P(EP, None, T),
            P(EP, None, T),
            P(EP, T, None),
            P(EP, None),
            P(EP, None),
        ),
        out_specs=P(EP, None),
        check_vma=False,
    )
```

```python
import functools
import jax
import jax.numpy as jnp
from jax import lax
from jax.experimental import pallas as pl
from jax.experimental.pallas import tpu as pltpu
from jax.sharding import Mesh
from jax.sharding import PartitionSpec as P


EP = ("ep_0", "ep_1", "ep_2")
Z, X, C, T = "ep_0", "ep_1", "ep_2", "tp"

eps = 1e-06
tau = 16.0
limit = 7.0
glu_alpha = 1.702
CAP = 3

f32 = jnp.float32
bf16 = jnp.bfloat16


def shift(value, axis, by):
    n = lax.axis_size(axis)
    return lax.ppermute(value, axis, [(i, (i + by) % n) for i in range(n)])


def order_of(n):
    return sorted(range(1, n), key=lambda s: (-min(s, n - s), s))


VMEM = pl.BlockSpec(memory_space=pltpu.VMEM)
SMEM = pl.BlockSpec(memory_space=pltpu.SMEM)
ANY = pl.BlockSpec(memory_space=pl.ANY)


def shaped(shape, dtype):
    return jax.ShapeDtypeStruct(shape, dtype)


def cost(flops, moved):
    return pl.CostEstimate(flops=int(flops), bytes_accessed=int(moved), transcendentals=0)


def pack_kernel(*refs):
    out, at = refs[-1], 0
    for ref in refs[:-1]:
        out[:, at : at + ref.shape[1]] = ref[...]
        at += ref.shape[1]


def pack(arrays):
    rows = arrays[0].shape[0]
    cols = sum(a.shape[1] for a in arrays)
    return pl.pallas_call(
        pack_kernel,
        out_shape=shaped((rows, cols), arrays[0].dtype),
        cost_estimate=cost(1e6, 4 * rows * cols),
        name="pack",
    )(*arrays)


def scale_kernel(tokens, gain, out, scale):
    values = tokens[...].astype(f32)
    meansq = jnp.mean(values * values, axis=-1, keepdims=True)
    scale[...] = jnp.broadcast_to(lax.rsqrt(meansq + eps), scale.shape)
    values = (values * gain[...].astype(f32)).astype(bf16)
    cols = out.shape[2]
    for i in range(out.shape[0]):
        out[i] = values[:, i * cols : (i + 1) * cols]


def scale(tokens, gain, nz):
    seqs, width = tokens.shape
    return pl.pallas_call(
        scale_kernel,
        out_shape=[shaped((nz, seqs, width // nz), bf16), shaped((seqs, 128), f32)],
        cost_estimate=cost(1e6, 4 * seqs * width),
        name="scale",
    )(tokens, gain[None])


def split_kernel(nz, where, down, *outs):
    nt = len(outs)
    chunk = outs[0].shape[1] // nz
    for s in range(nt):
        other = lax.rem(where[3] + s, nt)
        for i in range(nz):
            at = pl.multiple_of((i * nt + other) * chunk, chunk)
            outs[s][:, i * chunk : (i + 1) * chunk] = down[:, pl.ds(at, chunk)]


def split(where, down, nz, nt):
    rows, cols = down.shape
    return pl.pallas_call(
        functools.partial(split_kernel, nz),
        out_shape=[shaped((rows, cols // nt), bf16)] * nt,
        in_specs=[SMEM, VMEM],
        out_specs=[VMEM] * nt,
        cost_estimate=cost(1e6, 4 * rows * cols),
        name="split",
    )(where, down)


def project_kernel(nz, nx, where, tok, *refs):
    own, other = refs[:nx], refs[nx : 2 * nx]
    outs = refs[2 * nx : 2 * nx + nz]
    weight, turned = refs[-2:]
    z, x, c = where[0], where[1], where[2]
    rows = own[0].shape[0]
    seqs = outs[0].shape[0]
    for i in range(nx):
        base = lax.rem(x - i + nx, nx) * (2 * rows)
        weight[pl.ds(pl.multiple_of(base + c * rows, rows), rows), :] = own[i][...]
        weight[pl.ds(pl.multiple_of(base + (1 - c) * rows, rows), rows), :] = other[i][...]
    for s in range(nz):
        turned[s * seqs : (s + 1) * seqs, :] = tok[lax.rem(z + s, nz)].astype(f32)
    total = jnp.dot(turned[...].astype(bf16), weight[...], preferred_element_type=f32)
    for s in range(nz):
        outs[s][...] = total[s * seqs : (s + 1) * seqs, :].astype(bf16)


def project(where, tok, own, other):
    nz, seqs, depth = tok.shape
    nx, cols = len(own), own[0].shape[1]
    return pl.pallas_call(
        functools.partial(project_kernel, nz, nx),
        out_shape=[shaped((seqs, cols), bf16)] * nz,
        in_specs=[SMEM] + [VMEM] * (1 + 2 * nx),
        out_specs=[VMEM] * nz,
        scratch_shapes=[pltpu.VMEM((depth, cols), bf16), pltpu.VMEM((nz * seqs, depth), f32)],
        cost_estimate=cost(2 * nz * seqs * depth * cols, 2 * depth * cols),
        name="project",
    )(where, tok, *own, *other)


def join_kernel(*refs):
    for i, ref in enumerate(refs[:-1]):
        refs[-1][i] = ref[...]


def join(arrays):
    shape = (len(arrays), *arrays[0].shape)
    return pl.pallas_call(
        join_kernel,
        out_shape=shaped(shape, arrays[0].dtype),
        cost_estimate=cost(1e6, 4 * len(arrays) * arrays[0].size),
        name="join",
    )(*arrays)


def mix_kernel(nx, where, gated, partner, *refs):
    blocks = refs[:nx]
    outs = refs[nx : 2 * nx]
    weight, sems = refs[-2:]
    z, x, t = where[0], where[1], where[3]
    pairs = weight.shape[1]
    copies = []
    for i in range(nx):
        for r in range(pairs):
            copy = pltpu.make_async_copy(
                blocks[i].at[r],
                weight.at[lax.rem(x - i + nx, nx), lax.rem(lax.div(z, 2) - r + pairs, pairs)],
                sems.at[i, r],
            )
            copy.start()
            copies.append(copy)
    rows = jnp.concatenate([gated[...], partner[...]], axis=0)
    for copy in copies:
        copy.wait()
    depth, cols = weight.shape[4], pairs * 2 * weight.shape[3]
    for s in range(nx):
        block = weight[lax.rem(t + s, nx)].reshape(cols, depth)
        outs[s][...] = lax.dot_general(
            rows, block, (((1,), (1,)), ((), ())), preferred_element_type=f32
        ).astype(bf16)


def mix(where, gated, partner, blocks):
    nx = len(blocks)
    pairs, two, rows, depth = blocks[0].shape
    cols = pairs * two * rows
    seqs = 2 * gated.shape[0]
    return pl.pallas_call(
        functools.partial(mix_kernel, nx),
        out_shape=[shaped((seqs, cols), bf16)] * nx,
        in_specs=[SMEM, VMEM, VMEM] + [ANY] * nx,
        out_specs=[VMEM] * nx,
        scratch_shapes=[
            pltpu.VMEM((nx, pairs, two, rows, depth), bf16),
            pltpu.SemaphoreType.DMA((nx, pairs)),
        ],
        cost_estimate=cost(2 * seqs * cols * nx * depth, 2 * cols * nx * depth),
        name="mix",
    )(where, gated, partner, *blocks)


def put_rows(values, wide):
    chunks = values.shape[1] // 128
    for j in range(chunks):
        wide[pl.ds(j, values.shape[0], stride=chunks), :] = values[:, j * 128 : (j + 1) * 128]
    return wide[...].astype(bf16)


def dispatch_kernel(nz, nt, where, tokens, gain, sender, mine, other, out, stream, wide):
    c, t = where[2], where[3]
    chunk = stream.shape[1] // nz
    half = chunk // 2
    first, second = mine[...].astype(f32), other[...].astype(f32)
    first, second = jnp.where(c == 0, first, second), jnp.where(c == 0, second, first)
    for i in range(nz):
        own = tokens[:, pl.ds(pl.multiple_of((i * nt + t) * chunk, chunk), chunk)]
        at = slice(i * half, (i + 1) * half)
        mixed = jnp.concatenate([first[:, at], second[:, at]], axis=1)
        stream[:, i * chunk : (i + 1) * chunk] = own.astype(f32) + mixed
    rows = jnp.dot(
        sender[...], (stream[...] * gain[t]).astype(bf16), preferred_element_type=f32
    )
    out[...] = put_rows(rows, wide)


def dispatch(where, tokens, gain, sender, mine, other, nz, nt):
    slots, seqs = sender.shape
    part = 2 * mine.shape[1]
    wide = slots * part // 128
    return pl.pallas_call(
        functools.partial(dispatch_kernel, nz, nt),
        out_shape=[shaped((wide, 128), bf16), shaped((seqs, part), f32)],
        in_specs=[SMEM] + [VMEM] * 5,
        out_specs=[VMEM] * 2,
        scratch_shapes=[pltpu.VMEM((wide, 128), f32)],
        cost_estimate=cost(2 * slots * seqs * part, 6 * slots * part),
        name="dispatch",
    )(where, tokens, gain, sender, mine, other)


def unpack_kernel(rows, out, wide):
    wide[...] = rows[...].astype(f32)
    chunks = out.shape[1] // 128
    for j in range(chunks):
        out[:, j * 128 : (j + 1) * 128] = wide[
            pl.ds(j, out.shape[0], stride=chunks), :
        ].astype(bf16)


def unpack(rows, slots):
    part = rows.shape[0] * 128 // slots
    return pl.pallas_call(
        unpack_kernel,
        out_shape=shaped((slots, part), bf16),
        scratch_shapes=[pltpu.VMEM(rows.shape, f32)],
        cost_estimate=cost(1e6, 4 * slots * part),
        name="unpack",
    )(rows)


def expert_kernel(steps, nt, last, where, inverse, w_gate, w_lin, *refs):
    count = len(steps)
    pieces, refs = refs[:count], refs[count:]
    if last:
        before, refs = refs[:3], refs[3:]
    outs, (gates, lins, sems) = refs[:-3], refs[-3:]
    t = where[3]
    copies = []
    for i, s in enumerate(steps):
        at = lax.rem(t - s + nt, nt)
        pair = (
            pltpu.make_async_copy(w_gate.at[:, at], gates.at[i], sems.at[i, 0]),
            pltpu.make_async_copy(w_lin.at[:, at], lins.at[i], sems.at[i, 1]),
        )
        for copy in pair:
            copy.start()
        copies.append(pair)
    if last:
        gate, lin, sumsq = before[0][...], before[1][...], before[2][:, :1]
    else:
        gate, lin, sumsq = 0.0, 0.0, 0.0
    units = w_gate.shape[-1]
    for i, s in enumerate(steps):
        at = lax.rem(t - s + nt, nt)
        piece = pieces[i][...]
        plain = piece.astype(f32) * inverse[at]
        sumsq = sumsq + jnp.sum(plain * plain, axis=-1, keepdims=True)
        copies[i][0].wait()
        gate = gate + jnp.dot(
            piece, gates[i].reshape(piece.shape[1], units), preferred_element_type=f32
        )
        copies[i][1].wait()
        lin = lin + jnp.dot(
            piece, lins[i].reshape(piece.shape[1], units), preferred_element_type=f32
        )
    if last:
        width = nt * pieces[0].shape[1]
        scale = lax.rsqrt(sumsq / width + eps)
        gate = jnp.minimum(gate * scale, limit)
        lin = jnp.clip(lin * scale, -limit, limit)
        outs[0][...] = (gate * jax.nn.sigmoid(glu_alpha * gate) * (lin + 1.0)).astype(bf16)
    else:
        outs[0][...] = gate
        outs[1][...] = lin
        outs[2][...] = jnp.broadcast_to(sumsq, outs[2].shape)


def expert(where, inverse, w_gate, w_lin, steps, pieces, before):
    nz, nt, chunk, units = w_gate.shape
    slots, part = pieces[0].shape
    last = before is not None
    out_shape = (
        [shaped((slots, units), bf16)]
        if last
        else [shaped((slots, units), f32)] * 2 + [shaped((slots, 128), f32)]
    )
    count = len(steps)
    return pl.pallas_call(
        functools.partial(expert_kernel, steps, nt, last),
        out_shape=out_shape,
        in_specs=[SMEM, VMEM, ANY, ANY] + [VMEM] * (count + (3 if last else 0)),
        out_specs=[VMEM] * len(out_shape),
        scratch_shapes=[
            pltpu.VMEM((count, nz, chunk, units), bf16),
            pltpu.VMEM((count, nz, chunk, units), bf16),
            pltpu.SemaphoreType.DMA((count, 2)),
        ],
        cost_estimate=cost(4 * count * slots * part * units, 4 * count * part * units),
        name="expert_last" if last else "expert_first",
    )(where, inverse, w_gate, w_lin, *pieces, *(before or ()))


def down_kernel(nt, *refs):
    acts, downs = refs[:nt], refs[nt : 2 * nt]
    out, wide = refs[2 * nt :]
    total = jnp.dot(acts[0][...], downs[0][...], preferred_element_type=f32)
    for s in range(1, nt):
        total = total + jnp.dot(acts[s][...], downs[s][...], preferred_element_type=f32)
    out[...] = put_rows(total, wide)


def down_sum(acts, downs):
    nt = len(acts)
    slots, units = acts[0].shape
    part = downs[0].shape[1]
    wide = slots * part // 128
    return pl.pallas_call(
        functools.partial(down_kernel, nt),
        out_shape=shaped((wide, 128), bf16),
        scratch_shapes=[pltpu.VMEM((wide, 128), f32)],
        cost_estimate=cost(2 * nt * slots * units * part, 2 * nt * units * part),
        name="down",
    )(*acts, *downs)


def combine_kernel(rows, weights, stream, out, wide):
    wide[...] = rows[...].astype(f32)
    seqs, part = out.shape
    chunks = part // 128
    slots = wide.shape[0] // chunks
    for j in range(chunks):
        values = wide[pl.ds(j, slots, stride=chunks), :].astype(bf16)
        sums = jnp.dot(weights[...], values, preferred_element_type=f32)
        routed = sums[:seqs] + sums[seqs : 2 * seqs] + sums[2 * seqs :]
        at = slice(j * 128, (j + 1) * 128)
        out[:, at] = (stream[:, at] + routed).astype(bf16)


def combine(rows, weights, stream):
    return pl.pallas_call(
        combine_kernel,
        out_shape=shaped(stream.shape, bf16),
        scratch_shapes=[pltpu.VMEM(rows.shape, f32)],
        cost_estimate=cost(2 * weights.size * stream.shape[1], 2 * rows.size),
        name="combine",
    )(rows, weights, stream)


def finish_kernel(nz, where, *refs):
    pieces, out = refs[:-1], refs[-1]
    nt = len(pieces)
    chunk = pieces[0].shape[1] // nz
    for s in range(nt):
        other = lax.rem(where[3] - s + nt, nt)
        for i in range(nz):
            at = pl.multiple_of((i * nt + other) * chunk, chunk)
            out[:, pl.ds(at, chunk)] = pieces[s][:, i * chunk : (i + 1) * chunk]


def finish(where, pieces, nz):
    seqs, part = pieces[0].shape
    return pl.pallas_call(
        functools.partial(finish_kernel, nz),
        out_shape=shaped((seqs, part * len(pieces)), bf16),
        in_specs=[SMEM] + [VMEM] * len(pieces),
        out_specs=VMEM,
        cost_estimate=cost(1e6, 4 * seqs * part * len(pieces)),
        name="finish",
    )(where, *pieces)


def attention(arrived, first_scale, decay_shift, state, head_gain, key_cols, val_cols):
    seq_dev, heads_dev, key_dim, val_dim = state.shape
    projected = functools.reduce(jnp.add, [a.astype(f32) for a in arrived]) * first_scale
    q_rows = projected[:, :key_cols].reshape(seq_dev, heads_dev, key_dim) * key_dim ** (-0.5)
    k_rows = projected[:, key_cols : 2 * key_cols].reshape(seq_dev, heads_dev, key_dim)
    decay_pre = projected[:, 2 * key_cols : 3 * key_cols]
    v_rows = projected[:, 3 * key_cols : 3 * key_cols + val_cols].reshape(
        seq_dev, heads_dev, val_dim
    )
    rgates = projected[:, 3 * key_cols + val_cols :].reshape(seq_dev, heads_dev, val_dim)
    log_decay = jax.nn.log_sigmoid(decay_pre) / tau + decay_shift
    new_state = (
        jnp.exp(log_decay.reshape(seq_dev, heads_dev, key_dim))[..., None] * state
        + k_rows[..., None] * v_rows[:, :, None, :]
    )
    read = jnp.einsum("shk,shkv->shv", q_rows, new_state)
    read_sq = jnp.mean(read * read, axis=-1, keepdims=True)
    gated = (
        read
        * lax.rsqrt(read_sq + eps)
        * head_gain.astype(f32).reshape(heads_dev, val_dim)
        * jax.nn.silu(rgates)
    )
    return gated.reshape(seq_dev, heads_dev * val_dim).astype(bf16)


def to_bf16(value):
    return lax.reduce_precision(value, 8, 7)


def routing(expert_ids, route_weight, n_ep):
    seq_dev, top = expert_ids.shape
    flat_ids = expert_ids.reshape(-1)
    onehot = (flat_ids[:, None] == jnp.arange(n_ep, dtype=jnp.int32)[None, :]).astype(jnp.int32)
    rank = jnp.sum((jnp.cumsum(onehot, axis=0) - onehot) * onehot, axis=1)
    slot_of = (flat_ids * CAP + rank).reshape(seq_dev, top)
    slots = n_ep * CAP
    hits = jnp.arange(slots, dtype=jnp.int32)[None, None, :] == slot_of[:, :, None]
    sender = jnp.sum(hits.astype(f32), axis=1).T.astype(bf16)
    weights = jnp.sum(jnp.where(hits, route_weight[:, :, None], 0.0), axis=1)
    high = to_bf16(weights)
    middle = to_bf16(weights - high)
    low = weights - high - middle
    return sender, jnp.concatenate([high, middle, low], axis=0).astype(bf16)


def on_device(
    tokens,
    norm_gain,
    w_query,
    w_key,
    w_value,
    w_rgate,
    w_decay,
    decay_shift,
    state,
    head_gain,
    w_out,
    ffn_gain,
    w_gate,
    w_lin,
    w_down,
    expert_ids,
    route_weight,
):
    width = tokens.shape[1]
    nz, nx, nt = lax.axis_size(Z), lax.axis_size(X), lax.axis_size(T)
    n_ep = lax.axis_size(EP)
    slots = n_ep * CAP
    part = width // nt
    chunk = part // nz
    where = jnp.stack([lax.axis_index(a) for a in (Z, X, C, T)]).astype(jnp.int32)

    packed = pack((w_query, w_key, w_decay, w_value, w_rgate))
    own = [packed] + [shift(packed, X, i) for i in range(1, nx)]
    other = [shift(packed, C, 1)]
    other += [shift(w, C, 1) for w in own[1:]]

    tok_parts, first_scale = scale(tokens, norm_gain, nz)
    tok = lax.all_to_all(tok_parts, Z, 0, 0, tiled=True)

    out_t = w_out.T
    near = lax.ppermute(out_t, Z, [(i, i ^ 1) for i in range(nz)])
    odd = lax.rem(lax.axis_index(Z), 2) == 1
    pair = jnp.where(odd, jnp.stack([near, out_t]), jnp.stack([out_t, near]))
    pairs = [pair] + [shift(pair, Z, 2 * i) for i in order_of(nz // 2)]
    pairs = [pairs[0]] + [pairs[1 + order_of(nz // 2).index(i)] for i in range(1, nz // 2)]
    out_z = join(pairs)
    blocks = [out_z] + [shift(out_z, X, i) for i in range(1, nx)]

    downs = split(where, w_down[0], nz, nt)
    downs = [downs[0]] + [shift(downs[s], T, s) for s in range(1, nt)]

    sender, weights = routing(expert_ids, route_weight, n_ep)
    gain_of = ffn_gain.astype(f32).reshape(nz, nt, chunk)
    gain_of = jnp.moveaxis(gain_of, 1, 0).reshape(nt, 1, part)
    inverse = 1.0 / gain_of

    parts = project(where, tok, own, other)
    arrived = [parts[0]] + [shift(parts[s], Z, s) for s in order_of(nz)]
    gated = attention(
        arrived,
        first_scale[:, :1],
        decay_shift,
        state,
        head_gain,
        w_query.shape[1],
        w_value.shape[1],
    )
    partner = shift(gated, C, 1)
    mixed = mix(where, gated, partner, blocks)
    mixed = [mixed[0]] + [shift(mixed[s], T, s) for s in range(1, nt)]
    seqs = gated.shape[0]
    mine = functools.reduce(jnp.add, [m[:seqs].astype(f32) for m in mixed]).astype(bf16)
    theirs = functools.reduce(jnp.add, [m[seqs:].astype(f32) for m in mixed]).astype(bf16)
    other_half = shift(theirs, C, 1)
    outbound, stream = dispatch(
        where, tokens, gain_of, sender, mine, other_half, nz, nt
    )
    rows = lax.all_to_all(outbound.reshape(n_ep, -1, 128), EP, 0, 0, tiled=True).reshape(-1, 128)
    rows = unpack(rows, slots)
    pieces = [rows] + [shift(rows, T, s) for s in range(1, nt)]
    gates = w_gate.reshape(nz, nt, chunk, -1)
    lins = w_lin.reshape(nz, nt, chunk, -1)
    steps = [s for s in range(nt) if s != nt // 2]
    before = expert(where, inverse, gates, lins, steps, [pieces[s] for s in steps], None)
    act = expert(where, inverse, gates, lins, [nt // 2], [pieces[nt // 2]], before)[0]
    acts = [act] + [shift(act, T, s) for s in range(1, nt)]
    done = down_sum(acts, downs)
    returned = lax.all_to_all(done.reshape(n_ep, -1, 128), EP, 0, 0, tiled=True).reshape(-1, 128)
    result = combine(returned, weights, stream)
    results = [result] + [shift(result, T, s) for s in range(1, nt)]
    return finish(where, results, nz)


def solution(mesh):
    sizes = dict(mesh.shape)
    torus = Mesh(
        mesh.devices.reshape(sizes.get("z", 8), sizes.get("x", 4), 2, sizes["tp"]),
        (Z, X, C, T),
    )
    return jax.shard_map(
        on_device,
        mesh=torus,
        in_specs=(
            P(EP, None),
            P(),
            P(EP, T),
            P(EP, T),
            P(EP, T),
            P(EP, T),
            P(EP, T),
            P(EP, T),
            P(EP, T, None, None),
            P(T),
            P(T, EP),
            P(),
            P(EP, None, T),
            P(EP, None, T),
            P(EP, T, None),
            P(EP, None),
            P(EP, None),
        ),
        out_specs=P(EP, None),
        check_vma=False,
    )
```

```python
import functools
import jax
import jax.numpy as jnp
from jax import lax
from jax.experimental import pallas as pl
from jax.experimental.pallas import tpu as pltpu
from jax.sharding import Mesh
from jax.sharding import PartitionSpec as P


EP = ("ep_0", "ep_1", "ep_2")
Z, X, C, T = "ep_0", "ep_1", "ep_2", "tp"

eps = 1e-06
tau = 16.0
limit = 7.0
glu_alpha = 1.702
CAP = 3

f32 = jnp.float32
bf16 = jnp.bfloat16


def shift(value, axis, by):
    n = lax.axis_size(axis)
    return lax.ppermute(value, axis, [(i, (i + by) % n) for i in range(n)])


VMEM = pl.BlockSpec(memory_space=pltpu.VMEM)
SMEM = pl.BlockSpec(memory_space=pltpu.SMEM)
ANY = pl.BlockSpec(memory_space=pl.ANY)


def shaped(shape, dtype):
    return jax.ShapeDtypeStruct(shape, dtype)


def cost(flops, moved):
    return pl.CostEstimate(flops=int(flops), bytes_accessed=int(moved), transcendentals=0)


def pack_kernel(*refs):
    out, at = refs[-1], 0
    for ref in refs[:-1]:
        out[:, at : at + ref.shape[1]] = ref[...]
        at += ref.shape[1]


def pack(arrays):
    rows = arrays[0].shape[0]
    cols = sum(a.shape[1] for a in arrays)
    return pl.pallas_call(
        pack_kernel,
        out_shape=shaped((rows, cols), arrays[0].dtype),
        cost_estimate=cost(1e6, 4 * rows * cols),
        name="pack",
    )(*arrays)


def scale_kernel(tokens, gain, weight, out, scale):
    values = tokens[...].astype(f32)
    seqs = values.shape[0]
    meansq = jnp.mean(values * values, axis=-1, keepdims=True)
    scale[...] = jnp.broadcast_to(lax.rsqrt(meansq + eps), scale.shape)
    values = (values * gain[...].astype(f32).reshape(1, -1)).astype(bf16)
    cols = out.shape[2]
    for i in range(out.shape[0]):
        out[i, :seqs] = values[:, i * cols : (i + 1) * cols]
        out[i, seqs:] = weight[...]


def scale(tokens, gain, weight, nz):
    seqs, width = tokens.shape
    return pl.pallas_call(
        scale_kernel,
        out_shape=[
            shaped((nz, seqs + weight.shape[0], width // nz), bf16),
            shaped((seqs, 128), f32),
        ],
        cost_estimate=cost(1e6, 4 * seqs * width),
        name="scale",
    )(tokens, gain, weight)


def split_kernel(nz, where, down, *outs):
    nt = len(outs)
    chunk = outs[0].shape[1] // nz
    for s in range(nt):
        other = lax.rem(where[3] + s, nt)
        for i in range(nz):
            at = pl.multiple_of((i * nt + other) * chunk, chunk)
            outs[s][:, i * chunk : (i + 1) * chunk] = down[:, pl.ds(at, chunk)]


def split(where, down, nz, nt):
    rows, cols = down.shape
    return pl.pallas_call(
        functools.partial(split_kernel, nz),
        out_shape=[shaped((rows, cols // nt), bf16)] * nt,
        in_specs=[SMEM, VMEM],
        out_specs=[VMEM] * nt,
        cost_estimate=cost(1e6, 4 * rows * cols),
        name="split",
    )(where, down)


def project_kernel(nx, where, tok, *refs):
    own, other = refs[:nx], refs[nx : 2 * nx]
    out, weight = refs[2 * nx :]
    x, c = where[1], where[2]
    rows = own[0].shape[0]
    nz, seqs, cols = out.shape
    for i in range(nx):
        base = lax.rem(x - i + nx, nx) * (2 * rows)
        weight[pl.ds(pl.multiple_of(base + c * rows, rows), rows), :] = own[i][...]
        weight[pl.ds(pl.multiple_of(base + (1 - c) * rows, rows), rows), :] = other[i][...]
    left = tok[:, :seqs].astype(f32).reshape(nz * seqs, tok.shape[2]).astype(bf16)
    total = jnp.dot(left, weight[...], preferred_element_type=f32)
    out[...] = total.reshape(nz, seqs, cols).astype(bf16)


def project(where, tok, seqs, own, other):
    nz, _, depth = tok.shape
    nx, cols = len(own), own[0].shape[1]
    return pl.pallas_call(
        functools.partial(project_kernel, nx),
        out_shape=shaped((nz, seqs, cols), bf16),
        in_specs=[SMEM] + [VMEM] * (1 + 2 * nx),
        out_specs=VMEM,
        scratch_shapes=[pltpu.VMEM((depth, cols), bf16)],
        cost_estimate=cost(2 * nz * seqs * depth * cols, 2 * depth * cols),
        name="project",
    )(where, tok, *own, *other)


def attend_kernel(heads, arrived, scale, shift_of, state, gain, out):
    total = jnp.sum(arrived[...].astype(f32), axis=0) * scale[:, :1]
    rows = total.shape[0]
    keys = shift_of.shape[1]
    vals = out.shape[1]
    dim, width = keys // heads, vals // heads
    query = total[:, :keys] * dim ** (-0.5)
    key = total[:, keys : 2 * keys]
    pre = total[:, 2 * keys : 3 * keys]
    value = total[:, 3 * keys : 3 * keys + vals]
    rgate = total[:, 3 * keys + vals :]
    log_sig = jnp.minimum(pre, 0.0) - jnp.log1p(jnp.exp(-jnp.abs(pre)))
    faded = query * jnp.exp(log_sig / tau + shift_of[...])
    product = query * key
    silu = rgate * jax.nn.sigmoid(rgate)
    for h in range(heads):
        at = slice(h * dim, (h + 1) * dim)
        turned = jnp.transpose(faded[:, at])
        reads = [
            jnp.sum(turned[:, s : s + 1] * state[s, h], axis=0, keepdims=True)
            for s in range(rows)
        ]
        cols = slice(h * width, (h + 1) * width)
        read = jnp.concatenate(reads, axis=0)
        read = read + jnp.sum(product[:, at], axis=-1, keepdims=True) * value[:, cols]
        meansq = jnp.mean(read * read, axis=-1, keepdims=True)
        out[:, cols] = (
            read
            * lax.rsqrt(meansq + eps)
            * gain[...].astype(f32).reshape(1, -1)[:, cols]
            * silu[:, cols]
        ).astype(bf16)


def attend(arrived, scale, decay_shift, state, head_gain):
    seqs, heads, dim, width = state.shape
    step = 8
    vals = heads * width
    return pl.pallas_call(
        functools.partial(attend_kernel, heads),
        grid=(seqs // step,),
        out_shape=shaped((seqs, vals), bf16),
        in_specs=[
            pl.BlockSpec((arrived.shape[0], step, arrived.shape[2]), lambda i: (0, i, 0)),
            pl.BlockSpec((step, scale.shape[1]), lambda i: (i, 0)),
            pl.BlockSpec((step, heads * dim), lambda i: (i, 0)),
            pl.BlockSpec((step, heads, dim, width), lambda i: (i, 0, 0, 0)),
            pl.BlockSpec((vals,), lambda i: (0,)),
        ],
        out_specs=pl.BlockSpec((step, vals), lambda i: (i, 0)),
        cost_estimate=cost(4 * state.size, 4 * state.size),
        name="attend",
    )(arrived, scale, decay_shift, state, head_gain)


def mix_kernel(nx, where, gated, partner, *refs):
    blocks = refs[:nx]
    outs = refs[nx : 2 * nx]
    weight, sems = refs[-2:]
    x, t = where[1], where[3]
    copies = []
    for i in range(nx):
        copy = pltpu.make_async_copy(
            blocks[i], weight.at[lax.rem(x - i + nx, nx)], sems.at[i]
        )
        copy.start()
        copies.append(copy)
    rows = jnp.concatenate([gated[...], partner[...]], axis=0)
    for copy in copies:
        copy.wait()
    _, nz, cols, depth = weight.shape
    for s in range(nx):
        block = weight[lax.rem(t + s, nx)].reshape(nz * cols, depth)
        outs[s][...] = lax.dot_general(
            rows, block, (((1,), (1,)), ((), ())), preferred_element_type=f32
        ).astype(bf16)


def mix(where, gated, partner, blocks):
    nx = len(blocks)
    nz, rows, depth = blocks[0].shape
    cols = nz * rows
    seqs = 2 * gated.shape[0]
    return pl.pallas_call(
        functools.partial(mix_kernel, nx),
        out_shape=[shaped((seqs, cols), bf16)] * nx,
        in_specs=[SMEM, VMEM, VMEM] + [ANY] * nx,
        out_specs=[VMEM] * nx,
        scratch_shapes=[
            pltpu.VMEM((nx, nz, rows, depth), bf16),
            pltpu.SemaphoreType.DMA((nx,)),
        ],
        cost_estimate=cost(2 * seqs * cols * nx * depth, 2 * cols * nx * depth),
        name="mix",
    )(where, gated, partner, *blocks)


def put_rows(values, wide):
    chunks = values.shape[1] // 128
    for j in range(chunks):
        wide[pl.ds(j, values.shape[0], stride=chunks), :] = values[:, j * 128 : (j + 1) * 128]
    return wide[...].astype(bf16)


def dispatch_kernel(nz, nt, where, tokens, gain, sender, mine, other, out, stream, wide):
    c, t = where[2], where[3]
    chunk = stream.shape[1] // nz
    half = chunk // 2
    first, second = mine[...].astype(f32), other[...].astype(f32)
    first, second = jnp.where(c == 0, first, second), jnp.where(c == 0, second, first)
    for i in range(nz):
        own = tokens[:, pl.ds(pl.multiple_of((i * nt + t) * chunk, chunk), chunk)]
        at = slice(i * half, (i + 1) * half)
        mixed = jnp.concatenate([first[:, at], second[:, at]], axis=1)
        stream[:, i * chunk : (i + 1) * chunk] = own.astype(f32) + mixed
    rows = jnp.dot(
        sender[...], (stream[...] * gain[t]).astype(bf16), preferred_element_type=f32
    )
    out[...] = put_rows(rows, wide)


def dispatch(where, tokens, gain, sender, mine, other, nz, nt):
    slots, seqs = sender.shape
    part = 2 * mine.shape[1]
    wide = slots * part // 128
    return pl.pallas_call(
        functools.partial(dispatch_kernel, nz, nt),
        out_shape=[shaped((wide, 128), bf16), shaped((seqs, part), f32)],
        in_specs=[SMEM] + [VMEM] * 5,
        out_specs=[VMEM] * 2,
        scratch_shapes=[pltpu.VMEM((wide, 128), f32)],
        cost_estimate=cost(2 * slots * seqs * part, 6 * slots * part),
        name="dispatch",
    )(where, tokens, gain, sender, mine, other)


def take_rows(rows, wide, slots):
    wide[...] = rows[...].astype(f32)
    chunks = wide.shape[0] // slots
    return jnp.concatenate(
        [wide[pl.ds(j, slots, stride=chunks), :] for j in range(chunks)], axis=1
    )


def pick_kernel(step, nt, where, w_gate, w_lin, gate, lin, sems):
    at = lax.rem(where[3] - step + nt, nt)
    copies = (
        pltpu.make_async_copy(w_gate.at[:, at], gate, sems.at[0]),
        pltpu.make_async_copy(w_lin.at[:, at], lin, sems.at[1]),
    )
    for copy in copies:
        copy.start()
    for copy in copies:
        copy.wait()


def pick(where, w_gate, w_lin, step):
    nz, nt, chunk, units = w_gate.shape
    return pl.pallas_call(
        functools.partial(pick_kernel, step, nt),
        out_shape=[shaped((nz, chunk, units), bf16)] * 2,
        in_specs=[SMEM, ANY, ANY],
        out_specs=[VMEM, VMEM],
        scratch_shapes=[pltpu.SemaphoreType.DMA((2,))],
        cost_estimate=cost(1e6, 8 * nz * chunk * units),
        name="pick",
    )(where, w_gate, w_lin)


def expert_first_kernel(steps, nt, slots, where, inverse, w_gate, w_lin, *refs):
    count = len(steps)
    pieces, refs = refs[:count], refs[count:]
    outs, (gates, lins, wide, sems) = refs[:3], refs[3:]
    t = where[3]
    copies = []
    for i, s in enumerate(steps):
        at = lax.rem(t - s + nt, nt)
        pair = (
            pltpu.make_async_copy(w_gate.at[:, at], gates.at[i], sems.at[i, 0]),
            pltpu.make_async_copy(w_lin.at[:, at], lins.at[i], sems.at[i, 1]),
        )
        for copy in pair:
            copy.start()
        copies.append(pair)
    gate, lin, sumsq = 0.0, 0.0, 0.0
    units = w_gate.shape[-1]
    for i, s in enumerate(steps):
        at = lax.rem(t - s + nt, nt)
        rows = take_rows(pieces[i], wide, slots)
        plain = rows * inverse[at]
        sumsq = sumsq + jnp.sum(plain * plain, axis=-1, keepdims=True)
        rows = rows.astype(bf16)
        copies[i][0].wait()
        gate = gate + jnp.dot(
            rows, gates[i].reshape(-1, units), preferred_element_type=f32
        )
        copies[i][1].wait()
        lin = lin + jnp.dot(rows, lins[i].reshape(-1, units), preferred_element_type=f32)
    outs[0][...] = gate
    outs[1][...] = lin
    outs[2][...] = jnp.broadcast_to(sumsq, outs[2].shape)


def expert_first(where, inverse, w_gate, w_lin, steps, pieces, slots):
    nz, nt, chunk, units = w_gate.shape
    count = len(steps)
    part = nz * chunk
    return pl.pallas_call(
        functools.partial(expert_first_kernel, steps, nt, slots),
        out_shape=[shaped((slots, units), f32)] * 2 + [shaped((slots, 128), f32)],
        in_specs=[SMEM, VMEM, ANY, ANY] + [VMEM] * count,
        out_specs=[VMEM] * 3,
        scratch_shapes=[
            pltpu.VMEM((count, nz, chunk, units), bf16),
            pltpu.VMEM((count, nz, chunk, units), bf16),
            pltpu.VMEM(pieces[0].shape, f32),
            pltpu.SemaphoreType.DMA((count, 2)),
        ],
        cost_estimate=cost(4 * count * slots * part * units, 4 * count * part * units),
        name="expert_first",
    )(where, inverse, w_gate, w_lin, *pieces)


def expert_last_kernel(step, nt, where, inverse, w_gate, w_lin, piece, *refs):
    gate, lin, sumsq, out, wide = refs
    slots, units = out.shape
    rows = take_rows(piece, wide, slots)
    plain = rows * inverse[lax.rem(where[3] - step + nt, nt)]
    meansq = (sumsq[:, :1] + jnp.sum(plain * plain, axis=-1, keepdims=True)) / (
        nt * rows.shape[1]
    )
    rows = rows.astype(bf16)
    scale = lax.rsqrt(meansq + eps)
    gated = gate[...] + jnp.dot(
        rows, w_gate[...].reshape(-1, units), preferred_element_type=f32
    )
    linear = lin[...] + jnp.dot(
        rows, w_lin[...].reshape(-1, units), preferred_element_type=f32
    )
    gated = jnp.minimum(gated * scale, limit)
    linear = jnp.clip(linear * scale, -limit, limit)
    out[...] = (gated * jax.nn.sigmoid(glu_alpha * gated) * (linear + 1.0)).astype(bf16)


def expert_last(where, inverse, w_gate, w_lin, step, nt, piece, before):
    slots, units = before[0].shape
    return pl.pallas_call(
        functools.partial(expert_last_kernel, step, nt),
        out_shape=shaped((slots, units), bf16),
        in_specs=[SMEM] + [VMEM] * 7,
        out_specs=VMEM,
        scratch_shapes=[pltpu.VMEM(piece.shape, f32)],
        cost_estimate=cost(4 * slots * w_gate.size, 4 * w_gate.size),
        name="expert_last",
    )(where, inverse, w_gate, w_lin, piece, *before)


def down_kernel(nt, *refs):
    acts, downs = refs[:nt], refs[nt : 2 * nt]
    out, wide = refs[2 * nt :]
    total = jnp.dot(acts[0][...], downs[0][...], preferred_element_type=f32)
    for s in range(1, nt):
        total = total + jnp.dot(acts[s][...], downs[s][...], preferred_element_type=f32)
    out[...] = put_rows(total, wide)


def down_sum(acts, downs):
    nt = len(acts)
    slots, units = acts[0].shape
    part = downs[0].shape[1]
    wide = slots * part // 128
    return pl.pallas_call(
        functools.partial(down_kernel, nt),
        out_shape=shaped((wide, 128), bf16),
        scratch_shapes=[pltpu.VMEM((wide, 128), f32)],
        cost_estimate=cost(2 * nt * slots * units * part, 2 * nt * units * part),
        name="down",
    )(*acts, *downs)


def combine_kernel(rows, weights, stream, out, wide):
    wide[...] = rows[...].astype(f32)
    seqs, part = out.shape
    chunks = part // 128
    slots = wide.shape[0] // chunks
    for j in range(chunks):
        values = wide[pl.ds(j, slots, stride=chunks), :].astype(bf16)
        sums = jnp.dot(weights[...], values, preferred_element_type=f32)
        routed = sums[:seqs] + sums[seqs : 2 * seqs] + sums[2 * seqs :]
        at = slice(j * 128, (j + 1) * 128)
        out[:, at] = (stream[:, at] + routed).astype(bf16)


def combine(rows, weights, stream):
    return pl.pallas_call(
        combine_kernel,
        out_shape=shaped(stream.shape, bf16),
        scratch_shapes=[pltpu.VMEM(rows.shape, f32)],
        cost_estimate=cost(2 * weights.size * stream.shape[1], 2 * rows.size),
        name="combine",
    )(rows, weights, stream)


def finish_kernel(nz, where, *refs):
    pieces, out = refs[:-1], refs[-1]
    nt = len(pieces)
    chunk = pieces[0].shape[1] // nz
    for s in range(nt):
        other = lax.rem(where[3] - s + nt, nt)
        for i in range(nz):
            at = pl.multiple_of((i * nt + other) * chunk, chunk)
            out[:, pl.ds(at, chunk)] = pieces[s][:, i * chunk : (i + 1) * chunk]


def finish(where, pieces, nz):
    seqs, part = pieces[0].shape
    return pl.pallas_call(
        functools.partial(finish_kernel, nz),
        out_shape=shaped((seqs, part * len(pieces)), bf16),
        in_specs=[SMEM] + [VMEM] * len(pieces),
        out_specs=VMEM,
        cost_estimate=cost(1e6, 4 * seqs * part * len(pieces)),
        name="finish",
    )(where, *pieces)


def to_bf16(value):
    return lax.reduce_precision(value, 8, 7)


def routing(expert_ids, route_weight, n_ep):
    seq_dev, top = expert_ids.shape
    flat_ids = expert_ids.reshape(-1)
    onehot = (flat_ids[:, None] == jnp.arange(n_ep, dtype=jnp.int32)[None, :]).astype(jnp.int32)
    rank = jnp.sum((jnp.cumsum(onehot, axis=0) - onehot) * onehot, axis=1)
    slot_of = (flat_ids * CAP + rank).reshape(seq_dev, top)
    slots = n_ep * CAP
    hits = jnp.arange(slots, dtype=jnp.int32)[None, None, :] == slot_of[:, :, None]
    sender = jnp.sum(hits.astype(f32), axis=1).T.astype(bf16)
    weights = jnp.sum(jnp.where(hits, route_weight[:, :, None], 0.0), axis=1)
    high = to_bf16(weights)
    middle = to_bf16(weights - high)
    low = weights - high - middle
    return sender, jnp.concatenate([high, middle, low], axis=0).astype(bf16)


def on_device(
    tokens,
    norm_gain,
    w_query,
    w_key,
    w_value,
    w_rgate,
    w_decay,
    decay_shift,
    state,
    head_gain,
    w_out,
    ffn_gain,
    w_gate,
    w_lin,
    w_down,
    expert_ids,
    route_weight,
):
    width = tokens.shape[1]
    nz, nx, nt = lax.axis_size(Z), lax.axis_size(X), lax.axis_size(T)
    n_ep = lax.axis_size(EP)
    slots = n_ep * CAP
    part = width // nt
    chunk = part // nz
    where = jnp.stack([lax.axis_index(a) for a in (Z, X, C, T)]).astype(jnp.int32)

    packed = pack((w_query, w_key, w_decay, w_value, w_rgate))
    own = [packed] + [shift(packed, X, i) for i in range(1, nx)]
    other = [shift(packed, C, 1)]
    other += [shift(w, C, 1) for w in own[1:]]

    seqs = tokens.shape[0]
    payload, first_scale = scale(tokens, norm_gain, w_out.T, nz)
    moved = lax.all_to_all(payload, Z, 0, 0, tiled=True)
    out_z = moved[:, seqs:]
    blocks = [out_z] + [shift(out_z, X, i) for i in range(1, nx)]

    downs = split(where, w_down[0], nz, nt)
    downs = [downs[0]] + [shift(downs[s], T, s) for s in range(1, nt)]

    sender, weights = routing(expert_ids, route_weight, n_ep)
    gain_of = ffn_gain.astype(f32).reshape(nz, nt, chunk)
    gain_of = jnp.moveaxis(gain_of, 1, 0).reshape(nt, 1, part)
    inverse = 1.0 / gain_of

    parts = project(where, moved, seqs, own, other)
    arrived = lax.all_to_all(parts, Z, 0, 0, tiled=True)
    gated = attend(arrived, first_scale, decay_shift, state, head_gain)
    partner = shift(gated, C, 1)
    mixed = mix(where, gated, partner, blocks)
    mixed = [mixed[0]] + [shift(mixed[s], T, s) for s in range(1, nt)]
    mine = functools.reduce(jnp.add, [m[:seqs].astype(f32) for m in mixed]).astype(bf16)
    theirs = functools.reduce(jnp.add, [m[seqs:].astype(f32) for m in mixed]).astype(bf16)
    other_half = shift(theirs, C, 1)
    outbound, stream = dispatch(
        where, tokens, gain_of, sender, mine, other_half, nz, nt
    )
    rows = lax.all_to_all(
        outbound.reshape(n_ep, -1, 128), EP, 0, 0, tiled=True
    ).reshape(-1, 128)
    pieces = [rows] + [shift(rows, T, s) for s in range(1, nt)]
    gates = w_gate.reshape(nz, nt, chunk, -1)
    lins = w_lin.reshape(nz, nt, chunk, -1)
    far = nt // 2
    picked = pick(where, gates, lins, far)
    steps = [s for s in range(nt) if s != far]
    before = expert_first(
        where, inverse, gates, lins, steps, [pieces[s] for s in steps], slots
    )
    act = expert_last(where, inverse, *picked, far, nt, pieces[far], before)
    acts = [act] + [shift(act, T, s) for s in range(1, nt)]
    done = down_sum(acts, downs)
    returned = lax.all_to_all(
        done.reshape(n_ep, -1, 128), EP, 0, 0, tiled=True
    ).reshape(-1, 128)
    result = combine(returned, weights, stream)
    results = [result] + [shift(result, T, s) for s in range(1, nt)]
    return finish(where, results, nz)


def solution(mesh):
    sizes = dict(mesh.shape)
    torus = Mesh(
        mesh.devices.reshape(sizes.get("z", 8), sizes.get("x", 4), 2, sizes["tp"]),
        (Z, X, C, T),
    )
    return jax.shard_map(
        on_device,
        mesh=torus,
        in_specs=(
            P(EP, None),
            P(),
            P(EP, T),
            P(EP, T),
            P(EP, T),
            P(EP, T),
            P(EP, T),
            P(EP, T),
            P(EP, T, None, None),
            P(T),
            P(T, EP),
            P(),
            P(EP, None, T),
            P(EP, None, T),
            P(EP, T, None),
            P(EP, None),
            P(EP, None),
        ),
        out_specs=P(EP, None),
        check_vma=False,
    )
```

```python
import functools
import jax
import jax.numpy as jnp
from jax import lax
from jax.experimental import pallas as pl
from jax.experimental.pallas import tpu as pltpu
from jax.sharding import Mesh
from jax.sharding import PartitionSpec as P


EP = ("ep_0", "ep_1", "ep_2")
Z, X, C, T = "ep_0", "ep_1", "ep_2", "tp"

eps = 1e-06
tau = 16.0
limit = 7.0
glu_alpha = 1.702
CAP = 3

f32 = jnp.float32
bf16 = jnp.bfloat16


def shift(value, axis, by):
    n = lax.axis_size(axis)
    return lax.ppermute(value, axis, [(i, (i + by) % n) for i in range(n)])


def order_of(n):
    return sorted(range(1, n), key=lambda s: (-min(s, n - s), s))


VMEM = pl.BlockSpec(memory_space=pltpu.VMEM)
SMEM = pl.BlockSpec(memory_space=pltpu.SMEM)
ANY = pl.BlockSpec(memory_space=pl.ANY)
HBM = pl.BlockSpec(memory_space=pltpu.MemorySpace.HBM)


def shaped(shape, dtype):
    return jax.ShapeDtypeStruct(shape, dtype)


def room(mib):
    return pltpu.CompilerParams(vmem_limit_bytes=mib << 20)


def cost(flops, moved):
    return pl.CostEstimate(flops=int(flops), bytes_accessed=int(moved), transcendentals=0)


def run(copies):
    for copy in copies:
        copy.start()
    for copy in copies:
        copy.wait()


def pack_kernel(*refs):
    count = len(refs) - 2
    out, sems = refs[count:]
    copies, at = [], 0
    for i, ref in enumerate(refs[:count]):
        cols = ref.shape[1]
        copies.append(pltpu.make_async_copy(ref, out.at[:, at : at + cols], sems.at[i]))
        at += cols
    run(copies)


def pack(arrays):
    rows = arrays[0].shape[0]
    cols = sum(a.shape[1] for a in arrays)
    return pl.pallas_call(
        pack_kernel,
        out_shape=shaped((rows, cols), arrays[0].dtype),
        in_specs=[HBM] * len(arrays),
        out_specs=VMEM,
        scratch_shapes=[pltpu.SemaphoreType.DMA((len(arrays),))],
        cost_estimate=cost(1e6, 4 * rows * cols),
        compiler_params=room(62),
        name="pack",
    )(*arrays)


def scale_kernel(tokens_at, gain_at, weight_at, out, scale, tokens, gain, weight, sems):
    run(
        [
            pltpu.make_async_copy(ref, to, sems.at[i])
            for i, (ref, to) in enumerate(
                ((tokens_at, tokens), (gain_at, gain), (weight_at, weight))
            )
        ]
    )
    values = tokens[...].astype(f32)
    seqs = values.shape[0]
    meansq = jnp.mean(values * values, axis=-1, keepdims=True)
    scale[...] = jnp.broadcast_to(lax.rsqrt(meansq + eps), scale.shape)
    values = (values * gain[...].astype(f32).reshape(1, -1)).astype(bf16)
    cols = out.shape[2]
    for i in range(out.shape[0]):
        out[i, :seqs] = values[:, i * cols : (i + 1) * cols]
        out[i, seqs:] = weight[...]


def scale(tokens, gain, weight, nz):
    seqs, width = tokens.shape
    return pl.pallas_call(
        scale_kernel,
        out_shape=[
            shaped((nz, seqs + weight.shape[0], width // nz), bf16),
            shaped((seqs, 128), f32),
        ],
        in_specs=[HBM] * 3,
        out_specs=[VMEM] * 2,
        scratch_shapes=[
            pltpu.VMEM(tokens.shape, bf16),
            pltpu.VMEM(gain.shape, bf16),
            pltpu.VMEM(weight.shape, bf16),
            pltpu.SemaphoreType.DMA((3,)),
        ],
        cost_estimate=cost(1e6, 4 * seqs * width),
        compiler_params=room(62),
        name="scale",
    )(tokens, gain, weight)


def split_kernel(nz, where, down, *refs):
    outs, sems = refs[:-1], refs[-1]
    nt = len(outs)
    chunk = outs[0].shape[1] // nz
    copies = []
    for s in range(nt):
        other = lax.rem(where[3] + s, nt)
        for i in range(nz):
            at = pl.multiple_of((i * nt + other) * chunk, chunk)
            copies.append(
                pltpu.make_async_copy(
                    down.at[:, pl.ds(at, chunk)],
                    outs[s].at[:, pl.ds(i * chunk, chunk)],
                    sems.at[s, i],
                )
            )
    run(copies)


def split(where, down, nz, nt):
    rows, cols = down.shape
    return pl.pallas_call(
        functools.partial(split_kernel, nz),
        out_shape=[shaped((rows, cols // nt), bf16)] * nt,
        in_specs=[SMEM, HBM],
        out_specs=[VMEM] * nt,
        scratch_shapes=[pltpu.SemaphoreType.DMA((nt, nz))],
        cost_estimate=cost(1e6, 4 * rows * cols),
        compiler_params=room(6),
        name="split",
    )(where, down)


def project_kernel(nx, where, tok, *refs):
    own, other = refs[:nx], refs[nx : 2 * nx]
    out, weight = refs[2 * nx :]
    x, c = where[1], where[2]
    rows = own[0].shape[0]
    nz, seqs, cols = out.shape
    for i in range(nx):
        base = lax.rem(x - i + nx, nx) * (2 * rows)
        weight[pl.ds(pl.multiple_of(base + c * rows, rows), rows), :] = own[i][...]
        weight[pl.ds(pl.multiple_of(base + (1 - c) * rows, rows), rows), :] = other[i][...]
    left = tok[:, :seqs].astype(f32).reshape(nz * seqs, tok.shape[2]).astype(bf16)
    total = jnp.dot(left, weight[...], preferred_element_type=f32)
    out[...] = total.reshape(nz, seqs, cols).astype(bf16)


def project(where, tok, seqs, own, other):
    nz, _, depth = tok.shape
    nx, cols = len(own), own[0].shape[1]
    return pl.pallas_call(
        functools.partial(project_kernel, nx),
        out_shape=shaped((nz, seqs, cols), bf16),
        in_specs=[SMEM] + [VMEM] * (1 + 2 * nx),
        out_specs=VMEM,
        scratch_shapes=[pltpu.VMEM((depth, cols), bf16)],
        cost_estimate=cost(2 * nz * seqs * depth * cols, 2 * depth * cols),
        compiler_params=room(10),
        name="project",
    )(where, tok, *own, *other)


def attend_kernel(step, arrived, scale, shift_of, state_at, gain, out, state, sems):
    seqs, heads = state.shape[:2]
    copies = [
        pltpu.make_async_copy(
            state_at.at[pl.ds(i * step, step)], state.at[pl.ds(i * step, step)], sems.at[i]
        )
        for i in range(seqs // step)
    ]
    for copy in copies:
        copy.start()
    total = jnp.sum(arrived[...].astype(f32), axis=0) * scale[:, :1]
    rows = step
    keys = shift_of.shape[1]
    vals = out.shape[1]
    dim, width = keys // heads, vals // heads
    query = total[:, :keys] * dim ** (-0.5)
    key = total[:, keys : 2 * keys]
    pre = total[:, 2 * keys : 3 * keys]
    value = total[:, 3 * keys : 3 * keys + vals]
    rgate = total[:, 3 * keys + vals :]
    log_sig = jnp.minimum(pre, 0.0) - jnp.log1p(jnp.exp(-jnp.abs(pre)))
    faded = query * jnp.exp(log_sig / tau + shift_of[...])
    product = query * key
    silu = rgate * jax.nn.sigmoid(rgate)
    turned = [jnp.transpose(faded[:, h * dim : (h + 1) * dim]) for h in range(heads)]
    reads = [[] for _ in range(heads)]
    for i in range(seqs // rows):
        copies[i].wait()
        for s in range(i * rows, (i + 1) * rows):
            for h in range(heads):
                reads[h].append(
                    jnp.sum(turned[h][:, s : s + 1] * state[s, h], axis=0, keepdims=True)
                )
    for h in range(heads):
        at = slice(h * dim, (h + 1) * dim)
        cols = slice(h * width, (h + 1) * width)
        read = jnp.concatenate(reads[h], axis=0)
        read = read + jnp.sum(product[:, at], axis=-1, keepdims=True) * value[:, cols]
        meansq = jnp.mean(read * read, axis=-1, keepdims=True)
        out[:, cols] = (
            read
            * lax.rsqrt(meansq + eps)
            * gain[...].astype(f32).reshape(1, -1)[:, cols]
            * silu[:, cols]
        ).astype(bf16)


def attend(arrived, scale, decay_shift, state, head_gain):
    seqs, heads, _, width = state.shape
    step = 8
    vals = heads * width
    return pl.pallas_call(
        functools.partial(attend_kernel, step),
        out_shape=shaped((seqs, vals), bf16),
        in_specs=[VMEM, VMEM, VMEM, HBM, VMEM],
        out_specs=VMEM,
        scratch_shapes=[
            pltpu.VMEM(state.shape, f32),
            pltpu.SemaphoreType.DMA((seqs // step,)),
        ],
        cost_estimate=cost(4 * state.size, 4 * state.size),
        compiler_params=room(52),
        name="attend",
    )(arrived, scale, decay_shift, state, head_gain)


def mix_kernel(nx, where, gated, partner, *refs):
    blocks = refs[:nx]
    outs = refs[nx : 2 * nx]
    weight, sems = refs[-2:]
    x, t = where[1], where[3]
    copies = []
    for i in range(nx):
        copy = pltpu.make_async_copy(
            blocks[i], weight.at[lax.rem(x - i + nx, nx)], sems.at[i]
        )
        copy.start()
        copies.append(copy)
    rows = jnp.concatenate([gated[...], partner[...]], axis=0)
    for copy in copies:
        copy.wait()
    _, nz, cols, depth = weight.shape
    for s in range(nx):
        block = weight[lax.rem(t + s, nx)].reshape(nz * cols, depth)
        outs[s][...] = lax.dot_general(
            rows, block, (((1,), (1,)), ((), ())), preferred_element_type=f32
        ).astype(bf16)


def mix(where, gated, partner, blocks):
    nx = len(blocks)
    nz, rows, depth = blocks[0].shape
    cols = nz * rows
    seqs = 2 * gated.shape[0]
    return pl.pallas_call(
        functools.partial(mix_kernel, nx),
        out_shape=[shaped((seqs, cols), bf16)] * nx,
        in_specs=[SMEM, VMEM, VMEM] + [ANY] * nx,
        out_specs=[VMEM] * nx,
        scratch_shapes=[
            pltpu.VMEM((nx, nz, rows, depth), bf16),
            pltpu.SemaphoreType.DMA((nx,)),
        ],
        cost_estimate=cost(2 * seqs * cols * nx * depth, 2 * cols * nx * depth),
        compiler_params=room(8),
        name="mix",
    )(where, gated, partner, *blocks)


def put_rows(values, wide):
    chunks = values.shape[1] // 128
    for j in range(chunks):
        wide[pl.ds(j, values.shape[0], stride=chunks), :] = values[:, j * 128 : (j + 1) * 128]
    return wide[...].astype(bf16)


def dispatch_kernel(nz, nt, where, tokens, gain, sender, mine, other, out, stream, wide):
    c, t = where[2], where[3]
    chunk = stream.shape[1] // nz
    half = chunk // 2
    first, second = mine[...].astype(f32), other[...].astype(f32)
    first, second = jnp.where(c == 0, first, second), jnp.where(c == 0, second, first)
    for i in range(nz):
        own = tokens[:, pl.ds(pl.multiple_of((i * nt + t) * chunk, chunk), chunk)]
        at = slice(i * half, (i + 1) * half)
        mixed = jnp.concatenate([first[:, at], second[:, at]], axis=1)
        stream[:, i * chunk : (i + 1) * chunk] = own.astype(f32) + mixed
    rows = jnp.dot(
        sender[...], (stream[...] * gain[t]).astype(bf16), preferred_element_type=f32
    )
    out[...] = put_rows(rows, wide)


def dispatch(where, tokens, gain, sender, mine, other, nz, nt):
    slots, seqs = sender.shape
    part = 2 * mine.shape[1]
    wide = slots * part // 128
    return pl.pallas_call(
        functools.partial(dispatch_kernel, nz, nt),
        out_shape=[shaped((wide, 128), bf16), shaped((seqs, part), f32)],
        in_specs=[SMEM] + [VMEM] * 5,
        out_specs=[VMEM] * 2,
        scratch_shapes=[pltpu.VMEM((wide, 128), f32)],
        cost_estimate=cost(2 * slots * seqs * part, 6 * slots * part),
        compiler_params=room(6),
        name="dispatch",
    )(where, tokens, gain, sender, mine, other)


def take_rows(rows, wide, slots):
    wide[...] = rows[...].astype(f32)
    chunks = wide.shape[0] // slots
    return jnp.concatenate(
        [wide[pl.ds(j, slots, stride=chunks), :] for j in range(chunks)], axis=1
    )


def pick_kernel(nt, where, w_gate, w_lin, *refs):
    outs, sems = refs[:nt], refs[nt]
    units = w_gate.shape[-1]
    copies = []
    for s in range(nt):
        at = lax.rem(where[3] - s + nt, nt)
        for k, ref in enumerate((w_gate, w_lin)):
            copy = pltpu.make_async_copy(
                ref.at[:, at], outs[s].at[:, :, pl.ds(k * units, units)], sems.at[s, k]
            )
            copy.start()
            copies.append(copy)
    for copy in copies:
        copy.wait()


def pick(where, w_gate, w_lin):
    nz, nt, chunk, units = w_gate.shape
    return pl.pallas_call(
        functools.partial(pick_kernel, nt),
        out_shape=[shaped((nz, chunk, 2 * units), bf16)] * nt,
        in_specs=[SMEM, HBM, HBM],
        out_specs=[VMEM] * nt,
        scratch_shapes=[pltpu.SemaphoreType.DMA((nt, 2))],
        cost_estimate=cost(1e6, 4 * w_gate.size),
        compiler_params=room(8),
        name="pick",
    )(where, w_gate, w_lin)


def expert_kernel(step, nt, first, last, where, inverse, weight, piece, *refs):
    if not first:
        before, refs = refs[:2], refs[2:]
    outs, wide = refs[:-1], refs[-1]
    slots = outs[0].shape[0]
    rows = take_rows(piece, wide, slots)
    plain = rows * inverse[lax.rem(where[3] - step + nt, nt)]
    plain = plain * plain
    part = rows.shape[1]
    sumsq = plain[:, :128]
    for j in range(1, part // 128):
        sumsq = sumsq + plain[:, j * 128 : (j + 1) * 128]
    total = jnp.dot(
        rows.astype(bf16), weight[...].reshape(part, -1), preferred_element_type=f32
    )
    if not first:
        total = total + before[0][...]
        sumsq = sumsq + before[1][...]
    if not last:
        outs[0][...] = total
        outs[1][...] = sumsq
        return
    units = outs[0].shape[1]
    meansq = jnp.sum(sumsq, axis=-1, keepdims=True) / (nt * part)
    total = total * lax.rsqrt(meansq + eps)
    gate = jnp.minimum(total[:, :units], limit)
    lin = jnp.clip(total[:, units:], -limit, limit)
    outs[0][...] = (gate * jax.nn.sigmoid(glu_alpha * gate) * (lin + 1.0)).astype(bf16)


def expert(where, inverse, weight, step, nt, piece, slots, before=(), last=False):
    units = weight.shape[-1]
    out_shape = (
        shaped((slots, units // 2), bf16)
        if last
        else [shaped((slots, units), f32), shaped((slots, 128), f32)]
    )
    return pl.pallas_call(
        functools.partial(expert_kernel, step, nt, not before, last),
        out_shape=out_shape,
        in_specs=[SMEM] + [VMEM] * (3 + len(before)),
        out_specs=VMEM if last else [VMEM] * 2,
        scratch_shapes=[pltpu.VMEM(piece.shape, f32)],
        cost_estimate=cost(2 * slots * weight.size, 2 * weight.size),
        compiler_params=room(8),
        name="expert",
    )(where, inverse, weight, piece, *before)


def down_kernel(nt, *refs):
    acts, downs = refs[:nt], refs[nt : 2 * nt]
    out, wide = refs[2 * nt :]
    total = jnp.dot(acts[0][...], downs[0][...], preferred_element_type=f32)
    for s in range(1, nt):
        total = total + jnp.dot(acts[s][...], downs[s][...], preferred_element_type=f32)
    out[...] = put_rows(total, wide)


def down_sum(acts, downs):
    nt = len(acts)
    slots, units = acts[0].shape
    part = downs[0].shape[1]
    wide = slots * part // 128
    return pl.pallas_call(
        functools.partial(down_kernel, nt),
        out_shape=shaped((wide, 128), bf16),
        scratch_shapes=[pltpu.VMEM((wide, 128), f32)],
        cost_estimate=cost(2 * nt * slots * units * part, 2 * nt * units * part),
        compiler_params=room(10),
        name="down",
    )(*acts, *downs)


def combine_kernel(rows, weights, stream, out, wide):
    wide[...] = rows[...].astype(f32)
    seqs, part = out.shape
    chunks = part // 128
    slots = wide.shape[0] // chunks
    for j in range(chunks):
        values = wide[pl.ds(j, slots, stride=chunks), :].astype(bf16)
        sums = jnp.dot(weights[...], values, preferred_element_type=f32)
        routed = sums[:seqs] + sums[seqs : 2 * seqs] + sums[2 * seqs :]
        at = slice(j * 128, (j + 1) * 128)
        out[:, at] = (stream[:, at] + routed).astype(bf16)


def combine(rows, weights, stream):
    return pl.pallas_call(
        combine_kernel,
        out_shape=shaped(stream.shape, bf16),
        scratch_shapes=[pltpu.VMEM(rows.shape, f32)],
        cost_estimate=cost(2 * weights.size * stream.shape[1], 2 * rows.size),
        compiler_params=room(4),
        name="combine",
    )(rows, weights, stream)


def finish_kernel(nz, where, *refs):
    pieces, out = refs[:-1], refs[-1]
    nt = len(pieces)
    chunk = pieces[0].shape[1] // nz
    for s in range(nt):
        other = lax.rem(where[3] - s + nt, nt)
        for i in range(nz):
            at = pl.multiple_of((i * nt + other) * chunk, chunk)
            out[:, pl.ds(at, chunk)] = pieces[s][:, i * chunk : (i + 1) * chunk]


def finish(where, pieces, nz):
    seqs, part = pieces[0].shape
    return pl.pallas_call(
        functools.partial(finish_kernel, nz),
        out_shape=shaped((seqs, part * len(pieces)), bf16),
        in_specs=[SMEM] + [VMEM] * len(pieces),
        out_specs=VMEM,
        cost_estimate=cost(1e6, 4 * seqs * part * len(pieces)),
        compiler_params=room(2),
        name="finish",
    )(where, *pieces)


def to_bf16(value):
    return lax.reduce_precision(value, 8, 7)


def routing(expert_ids, route_weight, n_ep):
    seq_dev, top = expert_ids.shape
    flat_ids = expert_ids.reshape(-1)
    onehot = (flat_ids[:, None] == jnp.arange(n_ep, dtype=jnp.int32)[None, :]).astype(jnp.int32)
    rank = jnp.sum((jnp.cumsum(onehot, axis=0) - onehot) * onehot, axis=1)
    slot_of = (flat_ids * CAP + rank).reshape(seq_dev, top)
    slots = n_ep * CAP
    hits = jnp.arange(slots, dtype=jnp.int32)[None, None, :] == slot_of[:, :, None]
    sender = jnp.sum(hits.astype(f32), axis=1).T.astype(bf16)
    weights = jnp.sum(jnp.where(hits, route_weight[:, :, None], 0.0), axis=1)
    high = to_bf16(weights)
    middle = to_bf16(weights - high)
    low = weights - high - middle
    return sender, jnp.concatenate([high, middle, low], axis=0).astype(bf16)


def on_device(
    tokens,
    norm_gain,
    w_query,
    w_key,
    w_value,
    w_rgate,
    w_decay,
    decay_shift,
    state,
    head_gain,
    w_out,
    ffn_gain,
    w_gate,
    w_lin,
    w_down,
    expert_ids,
    route_weight,
):
    width = tokens.shape[1]
    nz, nx, nt = lax.axis_size(Z), lax.axis_size(X), lax.axis_size(T)
    n_ep = lax.axis_size(EP)
    slots = n_ep * CAP
    part = width // nt
    chunk = part // nz
    where = jnp.stack([lax.axis_index(a) for a in (Z, X, C, T)]).astype(jnp.int32)

    packed = pack((w_query, w_key, w_decay, w_value, w_rgate))
    own = [packed] + [shift(packed, X, i) for i in range(1, nx)]
    other = [shift(packed, C, 1)]
    other += [shift(w, C, 1) for w in own[1:]]

    seqs = tokens.shape[0]
    payload, first_scale = scale(tokens, norm_gain, w_out.T, nz)
    moved = lax.all_to_all(payload, Z, 0, 0, tiled=True)
    out_z = moved[:, seqs:]
    blocks = [out_z] + [shift(out_z, X, i) for i in range(1, nx)]

    downs = split(where, w_down[0], nz, nt)
    downs = [downs[0]] + [shift(downs[s], T, s) for s in range(1, nt)]

    sender, weights = routing(expert_ids, route_weight, n_ep)
    gain_of = ffn_gain.astype(f32).reshape(nz, nt, chunk)
    gain_of = jnp.moveaxis(gain_of, 1, 0).reshape(nt, 1, part)
    inverse = 1.0 / gain_of

    parts = project(where, moved, seqs, own, other)
    arrived = lax.all_to_all(parts, Z, 0, 0, tiled=True)
    gated = attend(arrived, first_scale, decay_shift, state, head_gain)
    partner = shift(gated, C, 1)
    mixed = mix(where, gated, partner, blocks)
    mixed = [mixed[0]] + [shift(mixed[s], T, s) for s in range(1, nt)]
    mine = functools.reduce(jnp.add, [m[:seqs].astype(f32) for m in mixed]).astype(bf16)
    theirs = functools.reduce(jnp.add, [m[seqs:].astype(f32) for m in mixed]).astype(bf16)
    other_half = shift(theirs, C, 1)
    outbound, stream = dispatch(
        where, tokens, gain_of, sender, mine, other_half, nz, nt
    )
    rows = lax.all_to_all(
        outbound.reshape(n_ep, -1, 128), EP, 0, 0, tiled=True
    ).reshape(-1, 128)
    pieces = [rows] + [shift(rows, T, s) for s in range(1, nt)]
    gates = w_gate.reshape(nz, nt, chunk, -1)
    lins = w_lin.reshape(nz, nt, chunk, -1)
    picked = pick(where, gates, lins)
    before = ()
    steps = [0] + order_of(nt)[1:] + [nt // 2]
    for s in steps:
        before = expert(
            where, inverse, picked[s], s, nt, pieces[s], slots, before, s == steps[-1]
        )
    act = before
    acts = [act] + [shift(act, T, s) for s in range(1, nt)]
    done = down_sum(acts, downs)
    returned = lax.all_to_all(
        done.reshape(n_ep, -1, 128), EP, 0, 0, tiled=True
    ).reshape(-1, 128)
    result = combine(returned, weights, stream)
    results = [result] + [shift(result, T, s) for s in range(1, nt)]
    return finish(where, results, nz)


def solution(mesh):
    sizes = dict(mesh.shape)
    torus = Mesh(
        mesh.devices.reshape(sizes.get("z", 8), sizes.get("x", 4), 2, sizes["tp"]),
        (Z, X, C, T),
    )
    return jax.shard_map(
        on_device,
        mesh=torus,
        in_specs=(
            P(EP, None),
            P(),
            P(EP, T),
            P(EP, T),
            P(EP, T),
            P(EP, T),
            P(EP, T),
            P(EP, T),
            P(EP, T, None, None),
            P(T),
            P(T, EP),
            P(),
            P(EP, None, T),
            P(EP, None, T),
            P(EP, T, None),
            P(EP, None),
            P(EP, None),
        ),
        out_specs=P(EP, None),
        check_vma=False,
    )
```

```python
import functools
import jax
import jax.numpy as jnp
from jax import lax
from jax.experimental import pallas as pl
from jax.experimental.pallas import tpu as pltpu
from jax.sharding import Mesh
from jax.sharding import PartitionSpec as P


EP = ("ep_0", "ep_1", "ep_2")
Z, X, C, T = "ep_0", "ep_1", "ep_2", "tp"

eps = 1e-06
tau = 16.0
limit = 7.0
glu_alpha = 1.702
CAP = 3

f32 = jnp.float32
bf16 = jnp.bfloat16


def shift(value, axis, by):
    n = lax.axis_size(axis)
    return lax.ppermute(value, axis, [(i, (i + by) % n) for i in range(n)])


def order_of(n):
    return sorted(range(1, n), key=lambda s: (-min(s, n - s), s))


VMEM = pl.BlockSpec(memory_space=pltpu.VMEM)
SMEM = pl.BlockSpec(memory_space=pltpu.SMEM)
ANY = pl.BlockSpec(memory_space=pl.ANY)
HBM = pl.BlockSpec(memory_space=pltpu.MemorySpace.HBM)


def shaped(shape, dtype):
    return jax.ShapeDtypeStruct(shape, dtype)


def room(mib):
    return pltpu.CompilerParams(vmem_limit_bytes=mib << 20)


def cost(flops, moved):
    return pl.CostEstimate(flops=int(flops), bytes_accessed=int(moved), transcendentals=0)


def run(copies):
    for copy in copies:
        copy.start()
    for copy in copies:
        copy.wait()


def pack_kernel(*refs):
    count = len(refs) - 2
    out, sems = refs[count:]
    copies, at = [], 0
    for i, ref in enumerate(refs[:count]):
        cols = ref.shape[1]
        copies.append(pltpu.make_async_copy(ref, out.at[:, at : at + cols], sems.at[i]))
        at += cols
    run(copies)


def pack(arrays):
    rows = arrays[0].shape[0]
    cols = sum(a.shape[1] for a in arrays)
    return pl.pallas_call(
        pack_kernel,
        out_shape=shaped((rows, cols), arrays[0].dtype),
        in_specs=[HBM] * len(arrays),
        out_specs=VMEM,
        scratch_shapes=[pltpu.SemaphoreType.DMA((len(arrays),))],
        cost_estimate=cost(1e6, 4 * rows * cols),
        compiler_params=room(62),
        name="pack",
    )(*arrays)


def scale_kernel(tokens_at, gain_at, weight_at, out, scale, tokens, gain, weight, sems):
    run(
        [
            pltpu.make_async_copy(ref, to, sems.at[i])
            for i, (ref, to) in enumerate(
                ((tokens_at, tokens), (gain_at, gain), (weight_at, weight))
            )
        ]
    )
    values = tokens[...].astype(f32)
    seqs = values.shape[0]
    meansq = jnp.mean(values * values, axis=-1, keepdims=True)
    scale[...] = jnp.broadcast_to(lax.rsqrt(meansq + eps), scale.shape)
    values = (values * gain[...].astype(f32).reshape(1, -1)).astype(bf16)
    cols = out.shape[2]
    for i in range(out.shape[0]):
        out[i, :seqs] = values[:, i * cols : (i + 1) * cols]
        out[i, seqs:] = weight[...]


def scale(tokens, gain, weight, nz):
    seqs, width = tokens.shape
    return pl.pallas_call(
        scale_kernel,
        out_shape=[
            shaped((nz, seqs + weight.shape[0], width // nz), bf16),
            shaped((seqs, 128), f32),
        ],
        in_specs=[HBM] * 3,
        out_specs=[VMEM] * 2,
        scratch_shapes=[
            pltpu.VMEM(tokens.shape, bf16),
            pltpu.VMEM(gain.shape, bf16),
            pltpu.VMEM(weight.shape, bf16),
            pltpu.SemaphoreType.DMA((3,)),
        ],
        cost_estimate=cost(1e6, 4 * seqs * width),
        compiler_params=room(62),
        name="scale",
    )(tokens, gain, weight)


def split_kernel(nz, where, down, *refs):
    outs, sems = refs[:-1], refs[-1]
    nt = len(outs)
    chunk = outs[0].shape[1] // nz
    copies = []
    for s in range(nt):
        other = lax.rem(where[3] + s, nt)
        for i in range(nz):
            at = pl.multiple_of((i * nt + other) * chunk, chunk)
            copies.append(
                pltpu.make_async_copy(
                    down.at[:, pl.ds(at, chunk)],
                    outs[s].at[:, pl.ds(i * chunk, chunk)],
                    sems.at[s, i],
                )
            )
    run(copies)


def split(where, down, nz, nt):
    rows, cols = down.shape
    return pl.pallas_call(
        functools.partial(split_kernel, nz),
        out_shape=[shaped((rows, cols // nt), bf16)] * nt,
        in_specs=[SMEM, HBM],
        out_specs=[VMEM] * nt,
        scratch_shapes=[pltpu.SemaphoreType.DMA((nt, nz))],
        cost_estimate=cost(1e6, 4 * rows * cols),
        compiler_params=room(62),
        name="split",
    )(where, down)


def project_kernel(nx, nz, where, tok, *refs):
    own, other = refs[:nx], refs[nx : 2 * nx]
    outs = refs[2 * nx : 2 * nx + nz]
    weight = refs[-1]
    z, x, c = where[0], where[1], where[2]
    rows = own[0].shape[0]
    seqs = outs[0].shape[0]
    for i in range(nx):
        base = lax.rem(x - i + nx, nx) * (2 * rows)
        weight[pl.ds(pl.multiple_of(base + c * rows, rows), rows), :] = own[i][...]
        weight[pl.ds(pl.multiple_of(base + (1 - c) * rows, rows), rows), :] = other[i][...]
    left = jnp.concatenate(
        [tok[lax.rem(z + s, nz), :seqs].astype(f32) for s in range(nz)], axis=0
    ).astype(bf16)
    total = jnp.dot(left, weight[...], preferred_element_type=f32)
    for s in range(nz):
        outs[s][...] = total[s * seqs : (s + 1) * seqs].astype(bf16)


def project(where, tok, seqs, own, other):
    nz, _, depth = tok.shape
    nx, cols = len(own), own[0].shape[1]
    return pl.pallas_call(
        functools.partial(project_kernel, nx, nz),
        out_shape=[shaped((seqs, cols), bf16)] * nz,
        in_specs=[SMEM] + [VMEM] * (1 + 2 * nx),
        out_specs=[VMEM] * nz,
        scratch_shapes=[pltpu.VMEM((depth, cols), bf16)],
        cost_estimate=cost(2 * nz * seqs * depth * cols, 2 * depth * cols),
        compiler_params=room(10),
        name="project",
    )(where, tok, *own, *other)


def attend_kernel(step, count, *refs):
    arrived, refs = refs[:count], refs[count:]
    scale, shift_of, state_at, gain, out, state, sems = refs
    seqs, heads = state.shape[:2]
    copies = [
        pltpu.make_async_copy(
            state_at.at[pl.ds(i * step, step)], state.at[pl.ds(i * step, step)], sems.at[i]
        )
        for i in range(seqs // step)
    ]
    for copy in copies:
        copy.start()
    total = arrived[0][...].astype(f32)
    for ref in arrived[1:]:
        total = total + ref[...].astype(f32)
    total = total * scale[:, :1]
    rows = step
    keys = shift_of.shape[1]
    vals = out.shape[1]
    dim, width = keys // heads, vals // heads
    query = total[:, :keys] * dim ** (-0.5)
    key = total[:, keys : 2 * keys]
    pre = total[:, 2 * keys : 3 * keys]
    value = total[:, 3 * keys : 3 * keys + vals]
    rgate = total[:, 3 * keys + vals :]
    log_sig = jnp.minimum(pre, 0.0) - jnp.log1p(jnp.exp(-jnp.abs(pre)))
    faded = query * jnp.exp(log_sig / tau + shift_of[...])
    product = query * key
    silu = rgate * jax.nn.sigmoid(rgate)
    turned = [jnp.transpose(faded[:, h * dim : (h + 1) * dim]) for h in range(heads)]
    reads = [[] for _ in range(heads)]
    for i in range(seqs // rows):
        copies[i].wait()
        for s in range(i * rows, (i + 1) * rows):
            for h in range(heads):
                reads[h].append(
                    jnp.sum(turned[h][:, s : s + 1] * state[s, h], axis=0, keepdims=True)
                )
    for h in range(heads):
        at = slice(h * dim, (h + 1) * dim)
        cols = slice(h * width, (h + 1) * width)
        read = jnp.concatenate(reads[h], axis=0)
        read = read + jnp.sum(product[:, at], axis=-1, keepdims=True) * value[:, cols]
        meansq = jnp.mean(read * read, axis=-1, keepdims=True)
        out[:, cols] = (
            read
            * lax.rsqrt(meansq + eps)
            * gain[...].astype(f32).reshape(1, -1)[:, cols]
            * silu[:, cols]
        ).astype(bf16)


def attend(arrived, scale, decay_shift, state, head_gain):
    seqs, heads, _, width = state.shape
    step = 8
    vals = heads * width
    return pl.pallas_call(
        functools.partial(attend_kernel, step, len(arrived)),
        out_shape=shaped((seqs, vals), bf16),
        in_specs=[VMEM] * (len(arrived) + 2) + [HBM, VMEM],
        out_specs=VMEM,
        scratch_shapes=[
            pltpu.VMEM(state.shape, f32),
            pltpu.SemaphoreType.DMA((seqs // step,)),
        ],
        cost_estimate=cost(4 * state.size, 4 * state.size),
        compiler_params=room(52),
        name="attend",
    )(*arrived, scale, decay_shift, state, head_gain)


def mix_kernel(nx, where, gated, partner, *refs):
    blocks = refs[:nx]
    outs = refs[nx : 2 * nx]
    weight, sems = refs[-2:]
    x, t = where[1], where[3]
    copies = []
    for i in range(nx):
        copy = pltpu.make_async_copy(
            blocks[i], weight.at[lax.rem(x - i + nx, nx)], sems.at[i]
        )
        copy.start()
        copies.append(copy)
    rows = jnp.concatenate([gated[...], partner[...]], axis=0)
    for copy in copies:
        copy.wait()
    _, nz, cols, depth = weight.shape
    for s in range(nx):
        block = weight[lax.rem(t + s, nx)].reshape(nz * cols, depth)
        outs[s][...] = lax.dot_general(
            rows, block, (((1,), (1,)), ((), ())), preferred_element_type=f32
        ).astype(bf16)


def mix(where, gated, partner, blocks):
    nx = len(blocks)
    nz, rows, depth = blocks[0].shape
    cols = nz * rows
    seqs = 2 * gated.shape[0]
    return pl.pallas_call(
        functools.partial(mix_kernel, nx),
        out_shape=[shaped((seqs, cols), bf16)] * nx,
        in_specs=[SMEM, VMEM, VMEM] + [ANY] * nx,
        out_specs=[VMEM] * nx,
        scratch_shapes=[
            pltpu.VMEM((nx, nz, rows, depth), bf16),
            pltpu.SemaphoreType.DMA((nx,)),
        ],
        cost_estimate=cost(2 * seqs * cols * nx * depth, 2 * cols * nx * depth),
        compiler_params=room(8),
        name="mix",
    )(where, gated, partner, *blocks)


def put_rows(values, wide):
    chunks = values.shape[1] // 128
    for j in range(chunks):
        wide[pl.ds(j, values.shape[0], stride=chunks), :] = values[:, j * 128 : (j + 1) * 128]
    return wide[...].astype(bf16)


def dispatch_kernel(nz, nt, where, tokens, gain, sender, mine, other, out, stream, wide):
    c, t = where[2], where[3]
    chunk = stream.shape[1] // nz
    half = chunk // 2
    first, second = mine[...].astype(f32), other[...].astype(f32)
    first, second = jnp.where(c == 0, first, second), jnp.where(c == 0, second, first)
    for i in range(nz):
        own = tokens[:, pl.ds(pl.multiple_of((i * nt + t) * chunk, chunk), chunk)]
        at = slice(i * half, (i + 1) * half)
        mixed = jnp.concatenate([first[:, at], second[:, at]], axis=1)
        stream[:, i * chunk : (i + 1) * chunk] = own.astype(f32) + mixed
    rows = jnp.dot(
        sender[...], (stream[...] * gain[t]).astype(bf16), preferred_element_type=f32
    )
    out[...] = put_rows(rows, wide)


def dispatch(where, tokens, gain, sender, mine, other, nz, nt):
    slots, seqs = sender.shape
    part = 2 * mine.shape[1]
    wide = slots * part // 128
    return pl.pallas_call(
        functools.partial(dispatch_kernel, nz, nt),
        out_shape=[shaped((wide, 128), bf16), shaped((seqs, part), f32)],
        in_specs=[SMEM] + [VMEM] * 5,
        out_specs=[VMEM] * 2,
        scratch_shapes=[pltpu.VMEM((wide, 128), f32)],
        cost_estimate=cost(2 * slots * seqs * part, 6 * slots * part),
        compiler_params=room(6),
        name="dispatch",
    )(where, tokens, gain, sender, mine, other)


def take_rows(rows, wide, slots):
    wide[...] = rows[...].astype(f32)
    chunks = wide.shape[0] // slots
    return jnp.concatenate(
        [wide[pl.ds(j, slots, stride=chunks), :] for j in range(chunks)], axis=1
    )


def pick_kernel(nt, where, w_gate, w_lin, *refs):
    outs, sems = refs[:nt], refs[nt]
    units = w_gate.shape[-1]
    copies = []
    for s in range(nt):
        at = lax.rem(where[3] - s + nt, nt)
        for k, ref in enumerate((w_gate, w_lin)):
            copy = pltpu.make_async_copy(
                ref.at[:, at], outs[s].at[:, :, pl.ds(k * units, units)], sems.at[s, k]
            )
            copy.start()
            copies.append(copy)
    for copy in copies:
        copy.wait()


def pick(where, w_gate, w_lin):
    nz, nt, chunk, units = w_gate.shape
    return pl.pallas_call(
        functools.partial(pick_kernel, nt),
        out_shape=[shaped((nz, chunk, 2 * units), bf16)] * nt,
        in_specs=[SMEM, HBM, HBM],
        out_specs=[VMEM] * nt,
        scratch_shapes=[pltpu.SemaphoreType.DMA((nt, 2))],
        cost_estimate=cost(1e6, 4 * w_gate.size),
        compiler_params=room(8),
        name="pick",
    )(where, w_gate, w_lin)


def expert_kernel(step, nt, first, last, where, inverse, weight, piece, *refs):
    if not first:
        before, refs = refs[:2], refs[2:]
    outs, wide = refs[:-1], refs[-1]
    slots = outs[0].shape[0]
    rows = take_rows(piece, wide, slots)
    plain = rows * inverse[lax.rem(where[3] - step + nt, nt)]
    plain = plain * plain
    part = rows.shape[1]
    sumsq = plain[:, :128]
    for j in range(1, part // 128):
        sumsq = sumsq + plain[:, j * 128 : (j + 1) * 128]
    total = jnp.dot(
        rows.astype(bf16), weight[...].reshape(part, -1), preferred_element_type=f32
    )
    if not first:
        total = total + before[0][...]
        sumsq = sumsq + before[1][...]
    if not last:
        outs[0][...] = total
        outs[1][...] = sumsq
        return
    units = outs[0].shape[1]
    meansq = jnp.sum(sumsq, axis=-1, keepdims=True) / (nt * part)
    total = total * lax.rsqrt(meansq + eps)
    gate = jnp.minimum(total[:, :units], limit)
    lin = jnp.clip(total[:, units:], -limit, limit)
    outs[0][...] = (gate * jax.nn.sigmoid(glu_alpha * gate) * (lin + 1.0)).astype(bf16)


def expert(where, inverse, weight, step, nt, piece, slots, before=(), last=False):
    units = weight.shape[-1]
    out_shape = (
        shaped((slots, units // 2), bf16)
        if last
        else [shaped((slots, units), f32), shaped((slots, 128), f32)]
    )
    return pl.pallas_call(
        functools.partial(expert_kernel, step, nt, not before, last),
        out_shape=out_shape,
        in_specs=[SMEM] + [VMEM] * (3 + len(before)),
        out_specs=VMEM if last else [VMEM] * 2,
        scratch_shapes=[pltpu.VMEM(piece.shape, f32)],
        cost_estimate=cost(2 * slots * weight.size, 2 * weight.size),
        compiler_params=room(8),
        name="expert",
    )(where, inverse, weight, piece, *before)


def down_kernel(nt, *refs):
    acts, downs = refs[:nt], refs[nt : 2 * nt]
    out, wide = refs[2 * nt :]
    total = jnp.dot(acts[0][...], downs[0][...], preferred_element_type=f32)
    for s in range(1, nt):
        total = total + jnp.dot(acts[s][...], downs[s][...], preferred_element_type=f32)
    out[...] = put_rows(total, wide)


def down_sum(acts, downs):
    nt = len(acts)
    slots, units = acts[0].shape
    part = downs[0].shape[1]
    wide = slots * part // 128
    return pl.pallas_call(
        functools.partial(down_kernel, nt),
        out_shape=shaped((wide, 128), bf16),
        scratch_shapes=[pltpu.VMEM((wide, 128), f32)],
        cost_estimate=cost(2 * nt * slots * units * part, 2 * nt * units * part),
        compiler_params=room(10),
        name="down",
    )(*acts, *downs)


def combine_kernel(rows, weights, stream, out, wide):
    wide[...] = rows[...].astype(f32)
    seqs, part = out.shape
    chunks = part // 128
    slots = wide.shape[0] // chunks
    for j in range(chunks):
        values = wide[pl.ds(j, slots, stride=chunks), :].astype(bf16)
        sums = jnp.dot(weights[...], values, preferred_element_type=f32)
        routed = sums[:seqs] + sums[seqs : 2 * seqs] + sums[2 * seqs :]
        at = slice(j * 128, (j + 1) * 128)
        out[:, at] = (stream[:, at] + routed).astype(bf16)


def combine(rows, weights, stream):
    return pl.pallas_call(
        combine_kernel,
        out_shape=shaped(stream.shape, bf16),
        scratch_shapes=[pltpu.VMEM(rows.shape, f32)],
        cost_estimate=cost(2 * weights.size * stream.shape[1], 2 * rows.size),
        compiler_params=room(4),
        name="combine",
    )(rows, weights, stream)


def finish_kernel(nz, where, *refs):
    pieces, out = refs[:-1], refs[-1]
    nt = len(pieces)
    chunk = pieces[0].shape[1] // nz
    for s in range(nt):
        other = lax.rem(where[3] - s + nt, nt)
        for i in range(nz):
            at = pl.multiple_of((i * nt + other) * chunk, chunk)
            out[:, pl.ds(at, chunk)] = pieces[s][:, i * chunk : (i + 1) * chunk]


def finish(where, pieces, nz):
    seqs, part = pieces[0].shape
    return pl.pallas_call(
        functools.partial(finish_kernel, nz),
        out_shape=shaped((seqs, part * len(pieces)), bf16),
        in_specs=[SMEM] + [VMEM] * len(pieces),
        out_specs=VMEM,
        cost_estimate=cost(1e6, 4 * seqs * part * len(pieces)),
        compiler_params=room(2),
        name="finish",
    )(where, *pieces)


def to_bf16(value):
    return lax.reduce_precision(value, 8, 7)


def routing(expert_ids, route_weight, n_ep):
    seq_dev, top = expert_ids.shape
    flat_ids = expert_ids.reshape(-1)
    onehot = (flat_ids[:, None] == jnp.arange(n_ep, dtype=jnp.int32)[None, :]).astype(jnp.int32)
    rank = jnp.sum((jnp.cumsum(onehot, axis=0) - onehot) * onehot, axis=1)
    slot_of = (flat_ids * CAP + rank).reshape(seq_dev, top)
    slots = n_ep * CAP
    hits = jnp.arange(slots, dtype=jnp.int32)[None, None, :] == slot_of[:, :, None]
    sender = jnp.sum(hits.astype(f32), axis=1).T.astype(bf16)
    weights = jnp.sum(jnp.where(hits, route_weight[:, :, None], 0.0), axis=1)
    high = to_bf16(weights)
    middle = to_bf16(weights - high)
    low = weights - high - middle
    return sender, jnp.concatenate([high, middle, low], axis=0).astype(bf16)


def on_device(
    tokens,
    norm_gain,
    w_query,
    w_key,
    w_value,
    w_rgate,
    w_decay,
    decay_shift,
    state,
    head_gain,
    w_out,
    ffn_gain,
    w_gate,
    w_lin,
    w_down,
    expert_ids,
    route_weight,
):
    width = tokens.shape[1]
    nz, nx, nt = lax.axis_size(Z), lax.axis_size(X), lax.axis_size(T)
    n_ep = lax.axis_size(EP)
    slots = n_ep * CAP
    part = width // nt
    chunk = part // nz
    where = jnp.stack([lax.axis_index(a) for a in (Z, X, C, T)]).astype(jnp.int32)

    packed = pack((w_query, w_key, w_decay, w_value, w_rgate))
    own = [packed] + [shift(packed, X, i) for i in range(1, nx)]
    other = [shift(packed, C, 1)]
    other += [shift(w, C, 1) for w in own[1:]]

    seqs = tokens.shape[0]
    payload, first_scale = scale(tokens, norm_gain, w_out.T, nz)
    moved = lax.all_to_all(payload, Z, 0, 0, tiled=True)
    out_z = moved[:, seqs:]
    blocks = [out_z] + [shift(out_z, X, i) for i in range(1, nx)]

    downs = split(where, w_down[0], nz, nt)
    downs = [downs[0]] + [shift(downs[s], T, s) for s in range(1, nt)]

    sender, weights = routing(expert_ids, route_weight, n_ep)
    gain_of = ffn_gain.astype(f32).reshape(nz, nt, chunk)
    gain_of = jnp.moveaxis(gain_of, 1, 0).reshape(nt, 1, part)
    inverse = 1.0 / gain_of

    parts = project(where, moved, seqs, own, other)
    arrived = [parts[0]] + [shift(parts[i], Z, i) for i in order_of(nz)]
    gated = attend(arrived, first_scale, decay_shift, state, head_gain)
    partner = shift(gated, C, 1)
    mixed = mix(where, gated, partner, blocks)
    mixed = [mixed[0]] + [shift(mixed[s], T, s) for s in range(1, nt)]
    mine = functools.reduce(jnp.add, [m[:seqs].astype(f32) for m in mixed]).astype(bf16)
    theirs = functools.reduce(jnp.add, [m[seqs:].astype(f32) for m in mixed]).astype(bf16)
    other_half = shift(theirs, C, 1)
    outbound, stream = dispatch(
        where, tokens, gain_of, sender, mine, other_half, nz, nt
    )
    rows = lax.all_to_all(
        outbound.reshape(n_ep, -1, 128), EP, 0, 0, tiled=True
    ).reshape(-1, 128)
    pieces = [rows] + [shift(rows, T, s) for s in range(1, nt)]
    gates = w_gate.reshape(nz, nt, chunk, -1)
    lins = w_lin.reshape(nz, nt, chunk, -1)
    picked = pick(where, gates, lins)
    before = ()
    steps = [0] + order_of(nt)[1:] + [nt // 2]
    for s in steps:
        before = expert(
            where, inverse, picked[s], s, nt, pieces[s], slots, before, s == steps[-1]
        )
    act = before
    acts = [act] + [shift(act, T, s) for s in range(1, nt)]
    done = down_sum(acts, downs)
    returned = lax.all_to_all(
        done.reshape(n_ep, -1, 128), EP, 0, 0, tiled=True
    ).reshape(-1, 128)
    result = combine(returned, weights, stream)
    results = [result] + [shift(result, T, s) for s in range(1, nt)]
    return finish(where, results, nz)


def solution(mesh):
    sizes = dict(mesh.shape)
    torus = Mesh(
        mesh.devices.reshape(sizes.get("z", 8), sizes.get("x", 4), 2, sizes["tp"]),
        (Z, X, C, T),
    )
    return jax.shard_map(
        on_device,
        mesh=torus,
        in_specs=(
            P(EP, None),
            P(),
            P(EP, T),
            P(EP, T),
            P(EP, T),
            P(EP, T),
            P(EP, T),
            P(EP, T),
            P(EP, T, None, None),
            P(T),
            P(T, EP),
            P(),
            P(EP, None, T),
            P(EP, None, T),
            P(EP, T, None),
            P(EP, None),
            P(EP, None),
        ),
        out_specs=P(EP, None),
        check_vma=False,
    )
```

```python
import functools
import jax
import jax.numpy as jnp
from jax import lax
from jax.experimental import pallas as pl
from jax.experimental.pallas import tpu as pltpu
from jax.sharding import Mesh
from jax.sharding import PartitionSpec as P


EP = ("ep_0", "ep_1", "ep_2")
Z, X, C, T = "ep_0", "ep_1", "ep_2", "tp"

eps = 1e-06
tau = 16.0
limit = 7.0
glu_alpha = 1.702
CAP = 3

f32 = jnp.float32
bf16 = jnp.bfloat16


def shift(value, axis, by):
    n = lax.axis_size(axis)
    return lax.ppermute(value, axis, [(i, (i + by) % n) for i in range(n)])


def order_of(n):
    return sorted(range(1, n), key=lambda s: (-min(s, n - s), s))


VMEM = pl.BlockSpec(memory_space=pltpu.VMEM)
SMEM = pl.BlockSpec(memory_space=pltpu.SMEM)
ANY = pl.BlockSpec(memory_space=pl.ANY)
HBM = pl.BlockSpec(memory_space=pltpu.MemorySpace.HBM)


def shaped(shape, dtype):
    return jax.ShapeDtypeStruct(shape, dtype)


def room(mib):
    return pltpu.CompilerParams(vmem_limit_bytes=mib << 20)


def cost(flops, moved):
    return pl.CostEstimate(flops=int(flops), bytes_accessed=int(moved), transcendentals=0)


def run(copies):
    for copy in copies:
        copy.start()
    for copy in copies:
        copy.wait()


def pack_kernel(*refs):
    count = len(refs) - 2
    out, sems = refs[count:]
    copies, at = [], 0
    for i, ref in enumerate(refs[:count]):
        cols = ref.shape[1]
        copies.append(pltpu.make_async_copy(ref, out.at[:, at : at + cols], sems.at[i]))
        at += cols
    run(copies)


def pack(arrays):
    rows = arrays[0].shape[0]
    cols = sum(a.shape[1] for a in arrays)
    return pl.pallas_call(
        pack_kernel,
        out_shape=shaped((rows, cols), arrays[0].dtype),
        in_specs=[HBM] * len(arrays),
        out_specs=VMEM,
        scratch_shapes=[pltpu.SemaphoreType.DMA((len(arrays),))],
        cost_estimate=cost(1e6, 4 * rows * cols),
        compiler_params=room(62),
        name="pack",
    )(*arrays)


def scale_kernel(tokens_at, gain_at, weight_at, out, scale, tokens, gain, weight, sems):
    run(
        [
            pltpu.make_async_copy(ref, to, sems.at[i])
            for i, (ref, to) in enumerate(
                ((tokens_at, tokens), (gain_at, gain), (weight_at, weight))
            )
        ]
    )
    values = tokens[...].astype(f32)
    seqs = values.shape[0]
    meansq = jnp.mean(values * values, axis=-1, keepdims=True)
    scale[...] = jnp.broadcast_to(lax.rsqrt(meansq + eps), scale.shape)
    values = (values * gain[...].astype(f32).reshape(1, -1)).astype(bf16)
    cols = out.shape[2]
    for i in range(out.shape[0]):
        out[i, :seqs] = values[:, i * cols : (i + 1) * cols]
        out[i, seqs:] = weight[...]


def scale(tokens, gain, weight, nz):
    seqs, width = tokens.shape
    return pl.pallas_call(
        scale_kernel,
        out_shape=[
            shaped((nz, seqs + weight.shape[0], width // nz), bf16),
            shaped((seqs, 128), f32),
        ],
        in_specs=[HBM] * 3,
        out_specs=[VMEM] * 2,
        scratch_shapes=[
            pltpu.VMEM(tokens.shape, bf16),
            pltpu.VMEM(gain.shape, bf16),
            pltpu.VMEM(weight.shape, bf16),
            pltpu.SemaphoreType.DMA((3,)),
        ],
        cost_estimate=cost(1e6, 4 * seqs * width),
        compiler_params=room(62),
        name="scale",
    )(tokens, gain, weight)


def split_kernel(nz, where, down, *refs):
    outs, sems = refs[:-1], refs[-1]
    nt = len(outs)
    chunk = outs[0].shape[1] // nz
    copies = []
    for s in range(nt):
        other = lax.rem(where[3] + s, nt)
        for i in range(nz):
            at = pl.multiple_of((i * nt + other) * chunk, chunk)
            copies.append(
                pltpu.make_async_copy(
                    down.at[:, pl.ds(at, chunk)],
                    outs[s].at[:, pl.ds(i * chunk, chunk)],
                    sems.at[s, i],
                )
            )
    run(copies)


def split(where, down, nz, nt):
    rows, cols = down.shape
    return pl.pallas_call(
        functools.partial(split_kernel, nz),
        out_shape=[shaped((rows, cols // nt), bf16)] * nt,
        in_specs=[SMEM, HBM],
        out_specs=[VMEM] * nt,
        scratch_shapes=[pltpu.SemaphoreType.DMA((nt, nz))],
        cost_estimate=cost(1e6, 4 * rows * cols),
        compiler_params=room(62),
        name="split",
    )(where, down)


def project_kernel(nx, nz, where, tok, *refs):
    own, other = refs[:nx], refs[nx : 2 * nx]
    outs = refs[2 * nx : 2 * nx + nz]
    weight = refs[-1]
    z, x, c = where[0], where[1], where[2]
    rows = own[0].shape[0]
    seqs = outs[0].shape[0]
    for i in range(nx):
        base = lax.rem(x - i + nx, nx) * (2 * rows)
        weight[pl.ds(pl.multiple_of(base + c * rows, rows), rows), :] = own[i][...]
        weight[pl.ds(pl.multiple_of(base + (1 - c) * rows, rows), rows), :] = other[i][...]
    left = jnp.concatenate(
        [tok[lax.rem(z + s, nz), :seqs].astype(f32) for s in range(nz)], axis=0
    ).astype(bf16)
    total = jnp.dot(left, weight[...], preferred_element_type=f32)
    for s in range(nz):
        outs[s][...] = total[s * seqs : (s + 1) * seqs].astype(bf16)


def project(where, tok, seqs, own, other):
    nz, _, depth = tok.shape
    nx, cols = len(own), own[0].shape[1]
    return pl.pallas_call(
        functools.partial(project_kernel, nx, nz),
        out_shape=[shaped((seqs, cols), bf16)] * nz,
        in_specs=[SMEM] + [VMEM] * (1 + 2 * nx),
        out_specs=[VMEM] * nz,
        scratch_shapes=[pltpu.VMEM((depth, cols), bf16)],
        cost_estimate=cost(2 * nz * seqs * depth * cols, 2 * depth * cols),
        compiler_params=room(10),
        name="project",
    )(where, tok, *own, *other)


def attend_kernel(step, count, *refs):
    arrived, refs = refs[:count], refs[count:]
    scale, shift_of, state_at, gain, out, state, sems = refs
    seqs, heads = state.shape[:2]
    copies = [
        pltpu.make_async_copy(
            state_at.at[pl.ds(i * step, step)], state.at[pl.ds(i * step, step)], sems.at[i]
        )
        for i in range(seqs // step)
    ]
    for copy in copies:
        copy.start()
    total = arrived[0][...].astype(f32)
    for ref in arrived[1:]:
        total = total + ref[...].astype(f32)
    total = total * scale[:, :1]
    rows = step
    keys = shift_of.shape[1]
    vals = out.shape[1]
    dim, width = keys // heads, vals // heads
    query = total[:, :keys] * dim ** (-0.5)
    key = total[:, keys : 2 * keys]
    pre = total[:, 2 * keys : 3 * keys]
    value = total[:, 3 * keys : 3 * keys + vals]
    rgate = total[:, 3 * keys + vals :]
    log_sig = jnp.minimum(pre, 0.0) - jnp.log1p(jnp.exp(-jnp.abs(pre)))
    faded = query * jnp.exp(log_sig / tau + shift_of[...])
    product = query * key
    silu = rgate * jax.nn.sigmoid(rgate)
    turned = [jnp.transpose(faded[:, h * dim : (h + 1) * dim]) for h in range(heads)]
    reads = [[] for _ in range(heads)]
    for i in range(seqs // rows):
        copies[i].wait()
        for s in range(i * rows, (i + 1) * rows):
            for h in range(heads):
                reads[h].append(
                    jnp.sum(turned[h][:, s : s + 1] * state[s, h], axis=0, keepdims=True)
                )
    for h in range(heads):
        at = slice(h * dim, (h + 1) * dim)
        cols = slice(h * width, (h + 1) * width)
        read = jnp.concatenate(reads[h], axis=0)
        read = read + jnp.sum(product[:, at], axis=-1, keepdims=True) * value[:, cols]
        meansq = jnp.mean(read * read, axis=-1, keepdims=True)
        out[:, cols] = (
            read
            * lax.rsqrt(meansq + eps)
            * gain[...].astype(f32).reshape(1, -1)[:, cols]
            * silu[:, cols]
        ).astype(bf16)


def attend(arrived, scale, decay_shift, state, head_gain):
    seqs, heads, _, width = state.shape
    step = 8
    vals = heads * width
    return pl.pallas_call(
        functools.partial(attend_kernel, step, len(arrived)),
        out_shape=shaped((seqs, vals), bf16),
        in_specs=[VMEM] * (len(arrived) + 2) + [HBM, VMEM],
        out_specs=VMEM,
        scratch_shapes=[
            pltpu.VMEM(state.shape, f32),
            pltpu.SemaphoreType.DMA((seqs // step,)),
        ],
        cost_estimate=cost(4 * state.size, 4 * state.size),
        compiler_params=room(52),
        name="attend",
    )(*arrived, scale, decay_shift, state, head_gain)


def mix_kernel(nx, where, gated, partner, *refs):
    blocks = refs[:nx]
    outs = refs[nx : 2 * nx]
    weight, sems = refs[-2:]
    x, t = where[1], where[3]
    copies = []
    for i in range(nx):
        copy = pltpu.make_async_copy(
            blocks[i], weight.at[lax.rem(x - i + nx, nx)], sems.at[i]
        )
        copy.start()
        copies.append(copy)
    rows = jnp.concatenate([gated[...], partner[...]], axis=0)
    for copy in copies:
        copy.wait()
    _, nz, cols, depth = weight.shape
    for s in range(nx):
        block = weight[lax.rem(t + s, nx)].reshape(nz * cols, depth)
        outs[s][...] = lax.dot_general(
            rows, block, (((1,), (1,)), ((), ())), preferred_element_type=f32
        ).astype(bf16)


def mix(where, gated, partner, blocks):
    nx = len(blocks)
    nz, rows, depth = blocks[0].shape
    cols = nz * rows
    seqs = 2 * gated.shape[0]
    return pl.pallas_call(
        functools.partial(mix_kernel, nx),
        out_shape=[shaped((seqs, cols), bf16)] * nx,
        in_specs=[SMEM, VMEM, VMEM] + [ANY] * nx,
        out_specs=[VMEM] * nx,
        scratch_shapes=[
            pltpu.VMEM((nx, nz, rows, depth), bf16),
            pltpu.SemaphoreType.DMA((nx,)),
        ],
        cost_estimate=cost(2 * seqs * cols * nx * depth, 2 * cols * nx * depth),
        compiler_params=room(8),
        name="mix",
    )(where, gated, partner, *blocks)


def put_rows(values, wide):
    chunks = values.shape[1] // 128
    for j in range(chunks):
        wide[pl.ds(j, values.shape[0], stride=chunks), :] = values[:, j * 128 : (j + 1) * 128]
    return wide[...].astype(bf16)


def dispatch_kernel(nz, nt, where, tokens, gain, sender, mine, other, out, stream, wide):
    c, t = where[2], where[3]
    chunk = stream.shape[1] // nz
    half = chunk // 2
    first, second = mine[...].astype(f32), other[...].astype(f32)
    first, second = jnp.where(c == 0, first, second), jnp.where(c == 0, second, first)
    for i in range(nz):
        own = tokens[:, pl.ds(pl.multiple_of((i * nt + t) * chunk, chunk), chunk)]
        at = slice(i * half, (i + 1) * half)
        mixed = jnp.concatenate([first[:, at], second[:, at]], axis=1)
        stream[:, i * chunk : (i + 1) * chunk] = own.astype(f32) + mixed
    rows = jnp.dot(
        sender[...], (stream[...] * gain[t]).astype(bf16), preferred_element_type=f32
    )
    out[...] = put_rows(rows, wide)


def dispatch(where, tokens, gain, sender, mine, other, nz, nt):
    slots, seqs = sender.shape
    part = 2 * mine.shape[1]
    wide = slots * part // 128
    return pl.pallas_call(
        functools.partial(dispatch_kernel, nz, nt),
        out_shape=[shaped((wide, 128), bf16), shaped((seqs, part), f32)],
        in_specs=[SMEM] + [VMEM] * 5,
        out_specs=[VMEM] * 2,
        scratch_shapes=[pltpu.VMEM((wide, 128), f32)],
        cost_estimate=cost(2 * slots * seqs * part, 6 * slots * part),
        compiler_params=room(6),
        name="dispatch",
    )(where, tokens, gain, sender, mine, other)


def take_rows(rows, wide, slots):
    wide[...] = rows[...].astype(f32)
    chunks = wide.shape[0] // slots
    return jnp.concatenate(
        [wide[pl.ds(j, slots, stride=chunks), :] for j in range(chunks)], axis=1
    )


def pick_kernel(nt, where, w_gate, w_lin, *refs):
    outs, sems = refs[:nt], refs[nt]
    units = w_gate.shape[-1]
    copies = []
    for s in range(nt):
        at = lax.rem(where[3] - s + nt, nt)
        for k, ref in enumerate((w_gate, w_lin)):
            copy = pltpu.make_async_copy(
                ref.at[:, at], outs[s].at[:, :, pl.ds(k * units, units)], sems.at[s, k]
            )
            copy.start()
            copies.append(copy)
    for copy in copies:
        copy.wait()


def pick(where, w_gate, w_lin):
    nz, nt, chunk, units = w_gate.shape
    return pl.pallas_call(
        functools.partial(pick_kernel, nt),
        out_shape=[shaped((nz, chunk, 2 * units), bf16)] * nt,
        in_specs=[SMEM, HBM, HBM],
        out_specs=[VMEM] * nt,
        scratch_shapes=[pltpu.SemaphoreType.DMA((nt, 2))],
        cost_estimate=cost(1e6, 4 * w_gate.size),
        compiler_params=room(8),
        name="pick",
    )(where, w_gate, w_lin)


def expert_kernel(step, nt, first, last, where, inverse, weight, piece, *refs):
    if not first:
        before, refs = refs[:2], refs[2:]
    outs, wide = refs[:-1], refs[-1]
    slots = outs[0].shape[0]
    rows = take_rows(piece, wide, slots)
    plain = rows * inverse[lax.rem(where[3] - step + nt, nt)]
    plain = plain * plain
    part = rows.shape[1]
    sumsq = plain[:, :128]
    for j in range(1, part // 128):
        sumsq = sumsq + plain[:, j * 128 : (j + 1) * 128]
    total = jnp.dot(
        rows.astype(bf16), weight[...].reshape(part, -1), preferred_element_type=f32
    )
    if not first:
        total = total + before[0][...]
        sumsq = sumsq + before[1][...]
    if not last:
        outs[0][...] = total
        outs[1][...] = sumsq
        return
    units = outs[0].shape[1]
    meansq = jnp.sum(sumsq, axis=-1, keepdims=True) / (nt * part)
    total = total * lax.rsqrt(meansq + eps)
    gate = jnp.minimum(total[:, :units], limit)
    lin = jnp.clip(total[:, units:], -limit, limit)
    outs[0][...] = (gate * jax.nn.sigmoid(glu_alpha * gate) * (lin + 1.0)).astype(bf16)


def expert(where, inverse, weight, step, nt, piece, slots, before=(), last=False):
    units = weight.shape[-1]
    out_shape = (
        shaped((slots, units // 2), bf16)
        if last
        else [shaped((slots, units), f32), shaped((slots, 128), f32)]
    )
    return pl.pallas_call(
        functools.partial(expert_kernel, step, nt, not before, last),
        out_shape=out_shape,
        in_specs=[SMEM] + [VMEM] * (3 + len(before)),
        out_specs=VMEM if last else [VMEM] * 2,
        scratch_shapes=[pltpu.VMEM(piece.shape, f32)],
        cost_estimate=cost(2 * slots * weight.size, 2 * weight.size),
        compiler_params=room(8),
        name="expert",
    )(where, inverse, weight, piece, *before)


def fetch_kernel(*refs):
    count = len(refs) - 2
    out, sems = refs[count:]
    rows = refs[0].shape[0]
    run(
        [
            pltpu.make_async_copy(ref, out.at[pl.ds(i * rows, rows)], sems.at[i])
            for i, ref in enumerate(refs[:count])
        ]
    )


def fetch(arrays):
    rows, cols = arrays[0].shape
    return pl.pallas_call(
        fetch_kernel,
        out_shape=shaped((rows * len(arrays), cols), bf16),
        in_specs=[HBM] * len(arrays),
        out_specs=VMEM,
        scratch_shapes=[pltpu.SemaphoreType.DMA((len(arrays),))],
        cost_estimate=cost(1e6, 4 * len(arrays) * rows * cols),
        compiler_params=room(4),
        name="fetch",
    )(*arrays)


def down_kernel(nt, *refs):
    acts = refs[:nt]
    weight, out, wide = refs[nt:]
    act = jnp.concatenate([ref[...] for ref in acts], axis=1)
    total = jnp.dot(act, weight[...], preferred_element_type=f32)
    out[...] = put_rows(total, wide)


def down_sum(acts, weight):
    nt = len(acts)
    slots, units = acts[0].shape
    part = weight.shape[1]
    wide = slots * part // 128
    return pl.pallas_call(
        functools.partial(down_kernel, nt),
        out_shape=shaped((wide, 128), bf16),
        scratch_shapes=[pltpu.VMEM((wide, 128), f32)],
        cost_estimate=cost(2 * nt * slots * units * part, 2 * nt * units * part),
        compiler_params=room(8),
        name="down",
    )(*acts, weight)


def combine_kernel(rows, weights, stream, out, wide):
    wide[...] = rows[...].astype(f32)
    seqs, part = out.shape
    chunks = part // 128
    slots = wide.shape[0] // chunks
    for j in range(chunks):
        values = wide[pl.ds(j, slots, stride=chunks), :].astype(bf16)
        sums = jnp.dot(weights[...], values, preferred_element_type=f32)
        routed = sums[:seqs] + sums[seqs : 2 * seqs] + sums[2 * seqs :]
        at = slice(j * 128, (j + 1) * 128)
        out[:, at] = (stream[:, at] + routed).astype(bf16)


def combine(rows, weights, stream):
    return pl.pallas_call(
        combine_kernel,
        out_shape=shaped(stream.shape, bf16),
        scratch_shapes=[pltpu.VMEM(rows.shape, f32)],
        cost_estimate=cost(2 * weights.size * stream.shape[1], 2 * rows.size),
        compiler_params=room(4),
        name="combine",
    )(rows, weights, stream)


def finish_kernel(nz, where, *refs):
    pieces, out = refs[:-1], refs[-1]
    nt = len(pieces)
    chunk = pieces[0].shape[1] // nz
    for s in range(nt):
        other = lax.rem(where[3] - s + nt, nt)
        for i in range(nz):
            at = pl.multiple_of((i * nt + other) * chunk, chunk)
            out[:, pl.ds(at, chunk)] = pieces[s][:, i * chunk : (i + 1) * chunk]


def finish(where, pieces, nz):
    seqs, part = pieces[0].shape
    return pl.pallas_call(
        functools.partial(finish_kernel, nz),
        out_shape=shaped((seqs, part * len(pieces)), bf16),
        in_specs=[SMEM] + [VMEM] * len(pieces),
        out_specs=VMEM,
        cost_estimate=cost(1e6, 4 * seqs * part * len(pieces)),
        compiler_params=room(2),
        name="finish",
    )(where, *pieces)


def to_bf16(value):
    return lax.reduce_precision(value, 8, 7)


def routing(expert_ids, route_weight, n_ep):
    seq_dev, top = expert_ids.shape
    flat_ids = expert_ids.reshape(-1)
    onehot = (flat_ids[:, None] == jnp.arange(n_ep, dtype=jnp.int32)[None, :]).astype(jnp.int32)
    rank = jnp.sum((jnp.cumsum(onehot, axis=0) - onehot) * onehot, axis=1)
    slot_of = (flat_ids * CAP + rank).reshape(seq_dev, top)
    slots = n_ep * CAP
    hits = jnp.arange(slots, dtype=jnp.int32)[None, None, :] == slot_of[:, :, None]
    sender = jnp.sum(hits.astype(f32), axis=1).T.astype(bf16)
    weights = jnp.sum(jnp.where(hits, route_weight[:, :, None], 0.0), axis=1)
    return sender, weights


def three_parts(weights):
    high = to_bf16(weights)
    middle = to_bf16(weights - high)
    low = weights - high - middle
    return jnp.concatenate([high, middle, low], axis=0).astype(bf16)


def on_device(
    tokens,
    norm_gain,
    w_query,
    w_key,
    w_value,
    w_rgate,
    w_decay,
    decay_shift,
    state,
    head_gain,
    w_out,
    ffn_gain,
    w_gate,
    w_lin,
    w_down,
    expert_ids,
    route_weight,
):
    width = tokens.shape[1]
    nz, nx, nt = lax.axis_size(Z), lax.axis_size(X), lax.axis_size(T)
    n_ep = lax.axis_size(EP)
    slots = n_ep * CAP
    part = width // nt
    chunk = part // nz
    where = jnp.stack([lax.axis_index(a) for a in (Z, X, C, T)]).astype(jnp.int32)

    packed = pack((w_query, w_key, w_decay, w_value, w_rgate))
    own = [packed] + [shift(packed, X, i) for i in range(1, nx)]
    other = [shift(packed, C, 1)]
    other += [shift(w, C, 1) for w in own[1:]]

    seqs = tokens.shape[0]
    payload, first_scale = scale(tokens, norm_gain, w_out.T, nz)
    moved = lax.all_to_all(payload, Z, 0, 0, tiled=True)
    out_z = moved[:, seqs:]
    blocks = [out_z] + [shift(out_z, X, i) for i in range(1, nx)]

    downs = split(where, w_down[0], nz, nt)
    downs = [downs[0]] + [shift(downs[s], T, s) for s in range(1, nt)]

    sender, weights = routing(expert_ids, route_weight, n_ep)
    gain_of = ffn_gain.astype(f32).reshape(nz, nt, chunk)
    gain_of = jnp.moveaxis(gain_of, 1, 0).reshape(nt, 1, part)
    inverse = 1.0 / gain_of
    weights = three_parts(weights)

    parts = project(where, moved, seqs, own, other)
    arrived = [parts[0]] + [shift(parts[i], Z, i) for i in order_of(nz)]
    gated = attend(arrived, first_scale, decay_shift, state, head_gain)
    partner = shift(gated, C, 1)
    mixed = mix(where, gated, partner, blocks)
    mixed = [mixed[0]] + [shift(mixed[s], T, s) for s in range(1, nt)]
    mine = functools.reduce(jnp.add, [m[:seqs].astype(f32) for m in mixed]).astype(bf16)
    theirs = functools.reduce(jnp.add, [m[seqs:].astype(f32) for m in mixed]).astype(bf16)
    other_half = shift(theirs, C, 1)
    outbound, stream = dispatch(
        where, tokens, gain_of, sender, mine, other_half, nz, nt
    )
    rows = lax.all_to_all(
        outbound.reshape(n_ep, -1, 128), EP, 0, 0, tiled=True
    ).reshape(-1, 128)
    pieces = [rows] + [shift(rows, T, s) for s in range(1, nt)]
    gates = w_gate.reshape(nz, nt, chunk, -1)
    lins = w_lin.reshape(nz, nt, chunk, -1)
    picked = pick(where, gates, lins)
    fetched = fetch(downs)
    before = ()
    steps = [0] + order_of(nt)[1:] + [nt // 2]
    for s in steps:
        before = expert(
            where, inverse, picked[s], s, nt, pieces[s], slots, before, s == steps[-1]
        )
    act = before
    acts = [act] + [shift(act, T, s) for s in range(1, nt)]
    done = down_sum(acts, fetched)
    returned = lax.all_to_all(
        done.reshape(n_ep, -1, 128), EP, 0, 0, tiled=True
    ).reshape(-1, 128)
    result = combine(returned, weights, stream)
    results = [result] + [shift(result, T, s) for s in range(1, nt)]
    return finish(where, results, nz)


def solution(mesh):
    sizes = dict(mesh.shape)
    torus = Mesh(
        mesh.devices.reshape(sizes.get("z", 8), sizes.get("x", 4), 2, sizes["tp"]),
        (Z, X, C, T),
    )
    return jax.shard_map(
        on_device,
        mesh=torus,
        in_specs=(
            P(EP, None),
            P(),
            P(EP, T),
            P(EP, T),
            P(EP, T),
            P(EP, T),
            P(EP, T),
            P(EP, T),
            P(EP, T, None, None),
            P(T),
            P(T, EP),
            P(),
            P(EP, None, T),
            P(EP, None, T),
            P(EP, T, None),
            P(EP, None),
            P(EP, None),
        ),
        out_specs=P(EP, None),
        check_vma=False,
    )
```

```python
import functools
import jax
import jax.numpy as jnp
from jax import lax
from jax.experimental import pallas as pl
from jax.experimental.pallas import tpu as pltpu
from jax.sharding import Mesh
from jax.sharding import PartitionSpec as P


EP = ("ep_0", "ep_1", "ep_2")
Z, X, C, T = "ep_0", "ep_1", "ep_2", "tp"

eps = 1e-06
tau = 16.0
limit = 7.0
glu_alpha = 1.702
CAP = 3

f32 = jnp.float32
bf16 = jnp.bfloat16


def shift(value, axis, by):
    n = lax.axis_size(axis)
    return lax.ppermute(value, axis, [(i, (i + by) % n) for i in range(n)])


def order_of(n):
    return sorted(range(1, n), key=lambda s: (-min(s, n - s), s))


VMEM = pl.BlockSpec(memory_space=pltpu.VMEM)
SMEM = pl.BlockSpec(memory_space=pltpu.SMEM)
ANY = pl.BlockSpec(memory_space=pl.ANY)
HBM = pl.BlockSpec(memory_space=pltpu.MemorySpace.HBM)


def shaped(shape, dtype):
    return jax.ShapeDtypeStruct(shape, dtype)


def room(mib):
    return pltpu.CompilerParams(vmem_limit_bytes=mib << 20)


def cost(flops, moved):
    return pl.CostEstimate(flops=int(flops), bytes_accessed=int(moved), transcendentals=0)


def run(copies):
    for copy in copies:
        copy.start()
    for copy in copies:
        copy.wait()


def pack_kernel(*refs):
    count = len(refs) - 2
    out, sems = refs[count:]
    copies, at = [], 0
    for i, ref in enumerate(refs[:count]):
        cols = ref.shape[1]
        copies.append(pltpu.make_async_copy(ref, out.at[:, at : at + cols], sems.at[i]))
        at += cols
    run(copies)


def pack(arrays):
    rows = arrays[0].shape[0]
    cols = sum(a.shape[1] for a in arrays)
    return pl.pallas_call(
        pack_kernel,
        out_shape=shaped((rows, cols), arrays[0].dtype),
        in_specs=[HBM] * len(arrays),
        out_specs=VMEM,
        scratch_shapes=[pltpu.SemaphoreType.DMA((len(arrays),))],
        cost_estimate=cost(1e6, 4 * rows * cols),
        compiler_params=room(62),
        name="pack",
    )(*arrays)


def scale_kernel(tokens_at, gain_at, weight_at, out, scale, tokens, gain, weight, sems):
    run(
        [
            pltpu.make_async_copy(ref, to, sems.at[i])
            for i, (ref, to) in enumerate(
                ((tokens_at, tokens), (gain_at, gain), (weight_at, weight))
            )
        ]
    )
    values = tokens[...].astype(f32)
    seqs = values.shape[0]
    meansq = jnp.mean(values * values, axis=-1, keepdims=True)
    scale[...] = jnp.broadcast_to(lax.rsqrt(meansq + eps), scale.shape)
    values = (values * gain[...].astype(f32).reshape(1, -1)).astype(bf16)
    cols = out.shape[2]
    for i in range(out.shape[0]):
        out[i, :seqs] = values[:, i * cols : (i + 1) * cols]
        out[i, seqs:] = weight[...]


def scale(tokens, gain, weight, nz):
    seqs, width = tokens.shape
    return pl.pallas_call(
        scale_kernel,
        out_shape=[
            shaped((nz, seqs + weight.shape[0], width // nz), bf16),
            shaped((seqs, 128), f32),
        ],
        in_specs=[HBM] * 3,
        out_specs=[VMEM] * 2,
        scratch_shapes=[
            pltpu.VMEM(tokens.shape, bf16),
            pltpu.VMEM(gain.shape, bf16),
            pltpu.VMEM(weight.shape, bf16),
            pltpu.SemaphoreType.DMA((3,)),
        ],
        cost_estimate=cost(1e6, 4 * seqs * width),
        compiler_params=room(62),
        name="scale",
    )(tokens, gain, weight)


def split_kernel(nz, where, down, *refs):
    outs, sems = refs[:-1], refs[-1]
    nt = len(outs)
    chunk = outs[0].shape[1] // nz
    copies = []
    for s in range(nt):
        other = lax.rem(where[3] + s, nt)
        for i in range(nz):
            at = pl.multiple_of((i * nt + other) * chunk, chunk)
            copies.append(
                pltpu.make_async_copy(
                    down.at[:, pl.ds(at, chunk)],
                    outs[s].at[:, pl.ds(i * chunk, chunk)],
                    sems.at[s, i],
                )
            )
    run(copies)


def split(where, down, nz, nt):
    rows, cols = down.shape
    return pl.pallas_call(
        functools.partial(split_kernel, nz),
        out_shape=[shaped((rows, cols // nt), bf16)] * nt,
        in_specs=[SMEM, HBM],
        out_specs=[VMEM] * nt,
        scratch_shapes=[pltpu.SemaphoreType.DMA((nt, nz))],
        cost_estimate=cost(1e6, 4 * rows * cols),
        compiler_params=room(62),
        name="split",
    )(where, down)


def project_kernel(nx, nz, where, tok, *refs):
    own, other = refs[:nx], refs[nx : 2 * nx]
    outs = refs[2 * nx : 2 * nx + nz]
    weight = refs[-1]
    z, x, c = where[0], where[1], where[2]
    rows = own[0].shape[0]
    seqs = outs[0].shape[0]
    for i in range(nx):
        base = lax.rem(x - i + nx, nx) * (2 * rows)
        weight[pl.ds(pl.multiple_of(base + c * rows, rows), rows), :] = own[i][...]
        weight[pl.ds(pl.multiple_of(base + (1 - c) * rows, rows), rows), :] = other[i][...]
    left = jnp.concatenate(
        [tok[lax.rem(z + s, nz), :seqs].astype(f32) for s in range(nz)], axis=0
    ).astype(bf16)
    total = jnp.dot(left, weight[...], preferred_element_type=f32)
    for s in range(nz):
        outs[s][...] = total[s * seqs : (s + 1) * seqs].astype(bf16)


def project(where, tok, seqs, own, other):
    nz, _, depth = tok.shape
    nx, cols = len(own), own[0].shape[1]
    return pl.pallas_call(
        functools.partial(project_kernel, nx, nz),
        out_shape=[shaped((seqs, cols), bf16)] * nz,
        in_specs=[SMEM] + [VMEM] * (1 + 2 * nx),
        out_specs=[VMEM] * nz,
        scratch_shapes=[pltpu.VMEM((depth, cols), bf16)],
        cost_estimate=cost(2 * nz * seqs * depth * cols, 2 * depth * cols),
        compiler_params=room(10),
        name="project",
    )(where, tok, *own, *other)


def attend_kernel(step, count, *refs):
    arrived, refs = refs[:count], refs[count:]
    scale, shift_of, state_at, gain, out, state, sems = refs
    seqs, heads = state.shape[:2]
    copies = [
        pltpu.make_async_copy(
            state_at.at[pl.ds(i * step, step)], state.at[pl.ds(i * step, step)], sems.at[i]
        )
        for i in range(seqs // step)
    ]
    for copy in copies:
        copy.start()
    total = arrived[0][...].astype(f32)
    for ref in arrived[1:]:
        total = total + ref[...].astype(f32)
    total = total * scale[:, :1]
    rows = step
    keys = shift_of.shape[1]
    vals = out.shape[1]
    dim, width = keys // heads, vals // heads
    query = total[:, :keys] * dim ** (-0.5)
    key = total[:, keys : 2 * keys]
    pre = total[:, 2 * keys : 3 * keys]
    value = total[:, 3 * keys : 3 * keys + vals]
    rgate = total[:, 3 * keys + vals :]
    log_sig = jnp.minimum(pre, 0.0) - jnp.log1p(jnp.exp(-jnp.abs(pre)))
    faded = query * jnp.exp(log_sig / tau + shift_of[...])
    product = query * key
    silu = rgate * jax.nn.sigmoid(rgate)
    turned = [jnp.transpose(faded[:, h * dim : (h + 1) * dim]) for h in range(heads)]
    reads = [[] for _ in range(heads)]
    for i in range(seqs // rows):
        copies[i].wait()
        for s in range(i * rows, (i + 1) * rows):
            for h in range(heads):
                reads[h].append(
                    jnp.sum(turned[h][:, s : s + 1] * state[s, h], axis=0, keepdims=True)
                )
    for h in range(heads):
        at = slice(h * dim, (h + 1) * dim)
        cols = slice(h * width, (h + 1) * width)
        read = jnp.concatenate(reads[h], axis=0)
        read = read + jnp.sum(product[:, at], axis=-1, keepdims=True) * value[:, cols]
        meansq = jnp.mean(read * read, axis=-1, keepdims=True)
        out[:, cols] = (
            read
            * lax.rsqrt(meansq + eps)
            * gain[...].astype(f32).reshape(1, -1)[:, cols]
            * silu[:, cols]
        ).astype(bf16)


def attend(arrived, scale, decay_shift, state, head_gain):
    seqs, heads, _, width = state.shape
    step = 8
    vals = heads * width
    return pl.pallas_call(
        functools.partial(attend_kernel, step, len(arrived)),
        out_shape=shaped((seqs, vals), bf16),
        in_specs=[VMEM] * (len(arrived) + 2) + [HBM, VMEM],
        out_specs=VMEM,
        scratch_shapes=[
            pltpu.VMEM(state.shape, f32),
            pltpu.SemaphoreType.DMA((seqs // step,)),
        ],
        cost_estimate=cost(4 * state.size, 4 * state.size),
        compiler_params=room(52),
        name="attend",
    )(*arrived, scale, decay_shift, state, head_gain)


def mix_kernel(nx, where, gated, partner, *refs):
    blocks = refs[:nx]
    outs = refs[nx : 2 * nx]
    weight, sems = refs[-2:]
    x, t = where[1], where[3]
    copies = []
    for i in range(nx):
        copy = pltpu.make_async_copy(
            blocks[i], weight.at[lax.rem(x - i + nx, nx)], sems.at[i]
        )
        copy.start()
        copies.append(copy)
    rows = jnp.concatenate([gated[...], partner[...]], axis=0)
    for copy in copies:
        copy.wait()
    _, nz, cols, depth = weight.shape
    for s in range(nx):
        block = weight[lax.rem(t + s, nx)].reshape(nz * cols, depth)
        outs[s][...] = lax.dot_general(
            rows, block, (((1,), (1,)), ((), ())), preferred_element_type=f32
        ).astype(bf16)


def mix(where, gated, partner, blocks):
    nx = len(blocks)
    nz, rows, depth = blocks[0].shape
    cols = nz * rows
    seqs = 2 * gated.shape[0]
    return pl.pallas_call(
        functools.partial(mix_kernel, nx),
        out_shape=[shaped((seqs, cols), bf16)] * nx,
        in_specs=[SMEM, VMEM, VMEM] + [ANY] * nx,
        out_specs=[VMEM] * nx,
        scratch_shapes=[
            pltpu.VMEM((nx, nz, rows, depth), bf16),
            pltpu.SemaphoreType.DMA((nx,)),
        ],
        cost_estimate=cost(2 * seqs * cols * nx * depth, 2 * cols * nx * depth),
        compiler_params=room(8),
        name="mix",
    )(where, gated, partner, *blocks)


def put_rows(values, wide):
    chunks = values.shape[1] // 128
    for j in range(chunks):
        wide[pl.ds(j, values.shape[0], stride=chunks), :] = values[:, j * 128 : (j + 1) * 128]
    return wide[...].astype(bf16)


def dispatch_kernel(nz, nt, where, tokens, gain, sender, mine, other, out, stream, wide):
    c, t = where[2], where[3]
    chunk = stream.shape[1] // nz
    half = chunk // 2
    first, second = mine[...].astype(f32), other[...].astype(f32)
    first, second = jnp.where(c == 0, first, second), jnp.where(c == 0, second, first)
    for i in range(nz):
        own = tokens[:, pl.ds(pl.multiple_of((i * nt + t) * chunk, chunk), chunk)]
        at = slice(i * half, (i + 1) * half)
        mixed = jnp.concatenate([first[:, at], second[:, at]], axis=1)
        stream[:, i * chunk : (i + 1) * chunk] = own.astype(f32) + mixed
    rows = jnp.dot(
        sender[...], (stream[...] * gain[t]).astype(bf16), preferred_element_type=f32
    )
    out[...] = put_rows(rows, wide)


def dispatch(where, tokens, gain, sender, mine, other, nz, nt):
    slots, seqs = sender.shape
    part = 2 * mine.shape[1]
    wide = slots * part // 128
    return pl.pallas_call(
        functools.partial(dispatch_kernel, nz, nt),
        out_shape=[shaped((wide, 128), bf16), shaped((seqs, part), f32)],
        in_specs=[SMEM] + [VMEM] * 5,
        out_specs=[VMEM] * 2,
        scratch_shapes=[pltpu.VMEM((wide, 128), f32)],
        cost_estimate=cost(2 * slots * seqs * part, 6 * slots * part),
        compiler_params=room(6),
        name="dispatch",
    )(where, tokens, gain, sender, mine, other)


def take_rows(rows, wide, slots):
    wide[...] = rows[...].astype(f32)
    chunks = wide.shape[0] // slots
    return jnp.concatenate(
        [wide[pl.ds(j, slots, stride=chunks), :] for j in range(chunks)], axis=1
    )


def pick_kernel(nt, where, w_gate, w_lin, *refs):
    outs, sems = refs[:nt], refs[nt]
    units = w_gate.shape[-1]
    copies = []
    for s in range(nt):
        at = lax.rem(where[3] - s + nt, nt)
        for k, ref in enumerate((w_gate, w_lin)):
            copy = pltpu.make_async_copy(
                ref.at[:, at], outs[s].at[:, :, pl.ds(k * units, units)], sems.at[s, k]
            )
            copy.start()
            copies.append(copy)
    for copy in copies:
        copy.wait()


def pick(where, w_gate, w_lin):
    nz, nt, chunk, units = w_gate.shape
    return pl.pallas_call(
        functools.partial(pick_kernel, nt),
        out_shape=[shaped((nz, chunk, 2 * units), bf16)] * nt,
        in_specs=[SMEM, HBM, HBM],
        out_specs=[VMEM] * nt,
        scratch_shapes=[pltpu.SemaphoreType.DMA((nt, 2))],
        cost_estimate=cost(1e6, 4 * w_gate.size),
        compiler_params=room(8),
        name="pick",
    )(where, w_gate, w_lin)


def expert_kernel(step, nt, first, last, where, inverse, weight, piece, *refs):
    if not first:
        before, refs = refs[:2], refs[2:]
    outs, wide = refs[:-1], refs[-1]
    slots = outs[0].shape[0]
    rows = take_rows(piece, wide, slots)
    plain = rows * inverse[lax.rem(where[3] - step + nt, nt)]
    plain = plain * plain
    part = rows.shape[1]
    sumsq = plain[:, :128]
    for j in range(1, part // 128):
        sumsq = sumsq + plain[:, j * 128 : (j + 1) * 128]
    total = jnp.dot(
        rows.astype(bf16), weight[...].reshape(part, -1), preferred_element_type=f32
    )
    if not first:
        total = total + before[0][...]
        sumsq = sumsq + before[1][...]
    if not last:
        outs[0][...] = total
        outs[1][...] = sumsq
        return
    units = outs[0].shape[1]
    meansq = jnp.sum(sumsq, axis=-1, keepdims=True) / (nt * part)
    total = total * lax.rsqrt(meansq + eps)
    gate = jnp.minimum(total[:, :units], limit)
    lin = jnp.clip(total[:, units:], -limit, limit)
    outs[0][...] = (gate * jax.nn.sigmoid(glu_alpha * gate) * (lin + 1.0)).astype(bf16)


def expert(where, inverse, weight, step, nt, piece, slots, before=(), last=False):
    units = weight.shape[-1]
    out_shape = (
        shaped((slots, units // 2), bf16)
        if last
        else [shaped((slots, units), f32), shaped((slots, 128), f32)]
    )
    return pl.pallas_call(
        functools.partial(expert_kernel, step, nt, not before, last),
        out_shape=out_shape,
        in_specs=[SMEM] + [VMEM] * (3 + len(before)),
        out_specs=VMEM if last else [VMEM] * 2,
        scratch_shapes=[pltpu.VMEM(piece.shape, f32)],
        cost_estimate=cost(2 * slots * weight.size, 2 * weight.size),
        compiler_params=room(8),
        name="expert",
    )(where, inverse, weight, piece, *before)


def fetch_kernel(*refs):
    count = len(refs) - 2
    out, sems = refs[count:]
    rows = refs[0].shape[0]
    run(
        [
            pltpu.make_async_copy(ref, out.at[pl.ds(i * rows, rows)], sems.at[i])
            for i, ref in enumerate(refs[:count])
        ]
    )


def fetch(arrays):
    rows, cols = arrays[0].shape
    return pl.pallas_call(
        fetch_kernel,
        out_shape=shaped((rows * len(arrays), cols), bf16),
        in_specs=[HBM] * len(arrays),
        out_specs=VMEM,
        scratch_shapes=[pltpu.SemaphoreType.DMA((len(arrays),))],
        cost_estimate=cost(1e6, 4 * len(arrays) * rows * cols),
        compiler_params=room(4),
        name="fetch",
    )(*arrays)


def down_kernel(nt, *refs):
    acts = refs[:nt]
    weight, out, wide = refs[nt:]
    act = jnp.concatenate([ref[...] for ref in acts], axis=1)
    total = jnp.dot(act, weight[...], preferred_element_type=f32)
    out[...] = put_rows(total, wide)


def down_sum(acts, weight):
    nt = len(acts)
    slots, units = acts[0].shape
    part = weight.shape[1]
    wide = slots * part // 128
    return pl.pallas_call(
        functools.partial(down_kernel, nt),
        out_shape=shaped((wide, 128), bf16),
        scratch_shapes=[pltpu.VMEM((wide, 128), f32)],
        cost_estimate=cost(2 * nt * slots * units * part, 2 * nt * units * part),
        compiler_params=room(8),
        name="down",
    )(*acts, weight)


def combine_kernel(rows, weights, stream, out, wide):
    wide[...] = rows[...].astype(f32)
    seqs, part = out.shape
    chunks = part // 128
    slots = wide.shape[0] // chunks
    for j in range(chunks):
        values = wide[pl.ds(j, slots, stride=chunks), :].astype(bf16)
        sums = jnp.dot(weights[...], values, preferred_element_type=f32)
        routed = sums[:seqs] + sums[seqs : 2 * seqs] + sums[2 * seqs :]
        at = slice(j * 128, (j + 1) * 128)
        out[:, at] = (stream[:, at] + routed).astype(bf16)


def combine(rows, weights, stream):
    return pl.pallas_call(
        combine_kernel,
        out_shape=shaped(stream.shape, bf16),
        scratch_shapes=[pltpu.VMEM(rows.shape, f32)],
        cost_estimate=cost(2 * weights.size * stream.shape[1], 2 * rows.size),
        compiler_params=room(4),
        name="combine",
    )(rows, weights, stream)


def finish_kernel(nz, where, *refs):
    pieces, out = refs[:-1], refs[-1]
    nt = len(pieces)
    chunk = pieces[0].shape[1] // nz
    for s in range(nt):
        other = lax.rem(where[3] - s + nt, nt)
        for i in range(nz):
            at = pl.multiple_of((i * nt + other) * chunk, chunk)
            out[:, pl.ds(at, chunk)] = pieces[s][:, i * chunk : (i + 1) * chunk]


def finish(where, pieces, nz):
    seqs, part = pieces[0].shape
    return pl.pallas_call(
        functools.partial(finish_kernel, nz),
        out_shape=shaped((seqs, part * len(pieces)), bf16),
        in_specs=[SMEM] + [VMEM] * len(pieces),
        out_specs=VMEM,
        cost_estimate=cost(1e6, 4 * seqs * part * len(pieces)),
        compiler_params=room(2),
        name="finish",
    )(where, *pieces)


def to_bf16(value):
    return lax.reduce_precision(value, 8, 7)


def routing(expert_ids, route_weight, n_ep):
    seq_dev, top = expert_ids.shape
    flat_ids = expert_ids.reshape(-1)
    onehot = (flat_ids[:, None] == jnp.arange(n_ep, dtype=jnp.int32)[None, :]).astype(jnp.int32)
    rank = jnp.sum((jnp.cumsum(onehot, axis=0) - onehot) * onehot, axis=1)
    slot_of = (flat_ids * CAP + rank).reshape(seq_dev, top)
    slots = n_ep * CAP
    hits = jnp.arange(slots, dtype=jnp.int32)[None, None, :] == slot_of[:, :, None]
    sender = jnp.sum(hits.astype(f32), axis=1).T.astype(bf16)
    weights = jnp.sum(jnp.where(hits, route_weight[:, :, None], 0.0), axis=1)
    return sender, weights


def three_parts(weights):
    high = to_bf16(weights)
    middle = to_bf16(weights - high)
    low = weights - high - middle
    return jnp.concatenate([high, middle, low], axis=0).astype(bf16)


def on_device(
    tokens,
    norm_gain,
    w_query,
    w_key,
    w_value,
    w_rgate,
    w_decay,
    decay_shift,
    state,
    head_gain,
    w_out,
    ffn_gain,
    w_gate,
    w_lin,
    w_down,
    expert_ids,
    route_weight,
):
    width = tokens.shape[1]
    nz, nx, nt = lax.axis_size(Z), lax.axis_size(X), lax.axis_size(T)
    n_ep = lax.axis_size(EP)
    slots = n_ep * CAP
    part = width // nt
    chunk = part // nz
    where = jnp.stack([lax.axis_index(a) for a in (Z, X, C, T)]).astype(jnp.int32)

    packed = pack((w_query, w_key, w_decay, w_value, w_rgate))
    own = [packed] + [shift(packed, X, i) for i in range(1, nx)]
    other = [shift(packed, C, 1)]
    other += [shift(w, C, 1) for w in own[1:]]

    seqs = tokens.shape[0]
    payload, first_scale = scale(tokens, norm_gain, w_out.T, nz)
    moved = lax.all_to_all(payload, Z, 0, 0, tiled=True)
    out_z = moved[:, seqs:]
    blocks = [out_z] + [None] * (nx - 1)
    for i in range(1, nx):
        blocks[i] = shift(out_z, X, i)

    downs = split(where, w_down[0], nz, nt)
    downs = [downs[0]] + [shift(downs[s], T, s) for s in range(1, nt)]

    sender, weights = routing(expert_ids, route_weight, n_ep)
    gain_of = ffn_gain.astype(f32).reshape(nz, nt, chunk)
    gain_of = jnp.moveaxis(gain_of, 1, 0).reshape(nt, 1, part)
    inverse = 1.0 / gain_of
    weights = three_parts(weights)

    parts = project(where, moved, seqs, own, other)
    arrived = [parts[0]]
    for i in order_of(nz):
        arrived.append(shift(parts[i], Z, i))
    gated = attend(arrived, first_scale, decay_shift, state, head_gain)
    partner = shift(gated, C, 1)
    mixed = mix(where, gated, partner, blocks)
    mixed = [mixed[0]] + [shift(mixed[s], T, s) for s in range(1, nt)]
    mine = functools.reduce(jnp.add, [m[:seqs].astype(f32) for m in mixed]).astype(bf16)
    theirs = functools.reduce(jnp.add, [m[seqs:].astype(f32) for m in mixed]).astype(bf16)
    other_half = shift(theirs, C, 1)
    outbound, stream = dispatch(
        where, tokens, gain_of, sender, mine, other_half, nz, nt
    )
    rows = lax.all_to_all(
        outbound.reshape(n_ep, -1, 128), EP, 0, 0, tiled=True
    ).reshape(-1, 128)
    pieces = [rows] + [shift(rows, T, s) for s in range(1, nt)]
    gates = w_gate.reshape(nz, nt, chunk, -1)
    lins = w_lin.reshape(nz, nt, chunk, -1)
    picked = pick(where, gates, lins)
    fetched = fetch(downs)
    before = ()
    steps = [0] + order_of(nt)[1:] + [nt // 2]
    for s in steps:
        before = expert(
            where, inverse, picked[s], s, nt, pieces[s], slots, before, s == steps[-1]
        )
    act = before
    acts = [act] + [shift(act, T, s) for s in range(1, nt)]
    done = down_sum(acts, fetched)
    returned = lax.all_to_all(
        done.reshape(n_ep, -1, 128), EP, 0, 0, tiled=True
    ).reshape(-1, 128)
    result = combine(returned, weights, stream)
    results = [result] + [shift(result, T, s) for s in range(1, nt)]
    return finish(where, results, nz)


def solution(mesh):
    sizes = dict(mesh.shape)
    torus = Mesh(
        mesh.devices.reshape(sizes.get("z", 8), sizes.get("x", 4), 2, sizes["tp"]),
        (Z, X, C, T),
    )
    return jax.shard_map(
        on_device,
        mesh=torus,
        in_specs=(
            P(EP, None),
            P(),
            P(EP, T),
            P(EP, T),
            P(EP, T),
            P(EP, T),
            P(EP, T),
            P(EP, T),
            P(EP, T, None, None),
            P(T),
            P(T, EP),
            P(),
            P(EP, None, T),
            P(EP, None, T),
            P(EP, T, None),
            P(EP, None),
            P(EP, None),
        ),
        out_specs=P(EP, None),
        check_vma=False,
    )
```

```python
import functools
import jax
import jax.numpy as jnp
from jax import lax
from jax.experimental import pallas as pl
from jax.experimental.pallas import tpu as pltpu
from jax.sharding import Mesh
from jax.sharding import PartitionSpec as P


EP = ("ep_0", "ep_1", "ep_2")
Z, X, C, T = "ep_0", "ep_1", "ep_2", "tp"

eps = 1e-06
tau = 16.0
limit = 7.0
glu_alpha = 1.702
CAP = 3

f32 = jnp.float32
bf16 = jnp.bfloat16


def shift(value, axis, by):
    n = lax.axis_size(axis)
    return lax.ppermute(value, axis, [(i, (i + by) % n) for i in range(n)])


def spread(values):
    n = len(values)
    out = [values[0]] + [None] * (n - 1)
    for s in sorted(range(1, n), key=lambda s: (-min(s, n - s), s)):
        out[s] = shift(values[s], T, s)
    return out


def order_of(n):
    return sorted(range(1, n), key=lambda s: (-min(s, n - s), s))


VMEM = pl.BlockSpec(memory_space=pltpu.VMEM)
SMEM = pl.BlockSpec(memory_space=pltpu.SMEM)
ANY = pl.BlockSpec(memory_space=pl.ANY)
HBM = pl.BlockSpec(memory_space=pltpu.MemorySpace.HBM)


def shaped(shape, dtype):
    return jax.ShapeDtypeStruct(shape, dtype)


def room(mib):
    return pltpu.CompilerParams(vmem_limit_bytes=mib << 20)


def cost(flops, moved):
    return pl.CostEstimate(flops=int(flops), bytes_accessed=int(moved), transcendentals=0)


def run(copies):
    for copy in copies:
        copy.start()
    for copy in copies:
        copy.wait()


def pack_kernel(*refs):
    count = len(refs) - 2
    out, sems = refs[count:]
    copies, at = [], 0
    for i, ref in enumerate(refs[:count]):
        cols = ref.shape[1]
        copies.append(pltpu.make_async_copy(ref, out.at[:, at : at + cols], sems.at[i]))
        at += cols
    run(copies)


def pack(arrays):
    rows = arrays[0].shape[0]
    cols = sum(a.shape[1] for a in arrays)
    return pl.pallas_call(
        pack_kernel,
        out_shape=shaped((rows, cols), arrays[0].dtype),
        in_specs=[HBM] * len(arrays),
        out_specs=VMEM,
        scratch_shapes=[pltpu.SemaphoreType.DMA((len(arrays),))],
        cost_estimate=cost(1e6, 4 * rows * cols),
        compiler_params=room(62),
        name="pack",
    )(*arrays)


def scale_kernel(tokens_at, gain_at, weight_at, out, scale, tokens, gain, weight, sems):
    run(
        [
            pltpu.make_async_copy(ref, to, sems.at[i])
            for i, (ref, to) in enumerate(
                ((tokens_at, tokens), (gain_at, gain), (weight_at, weight))
            )
        ]
    )
    values = tokens[...].astype(f32)
    seqs = values.shape[0]
    meansq = jnp.mean(values * values, axis=-1, keepdims=True)
    scale[...] = jnp.broadcast_to(lax.rsqrt(meansq + eps), scale.shape)
    values = (values * gain[...].astype(f32).reshape(1, -1)).astype(bf16)
    cols = out.shape[2]
    for i in range(out.shape[0]):
        out[i, :seqs] = values[:, i * cols : (i + 1) * cols]
        out[i, seqs:] = weight[...]


def scale(tokens, gain, weight, nz):
    seqs, width = tokens.shape
    return pl.pallas_call(
        scale_kernel,
        out_shape=[
            shaped((nz, seqs + weight.shape[0], width // nz), bf16),
            shaped((seqs, 128), f32),
        ],
        in_specs=[HBM] * 3,
        out_specs=[VMEM] * 2,
        scratch_shapes=[
            pltpu.VMEM(tokens.shape, bf16),
            pltpu.VMEM(gain.shape, bf16),
            pltpu.VMEM(weight.shape, bf16),
            pltpu.SemaphoreType.DMA((3,)),
        ],
        cost_estimate=cost(1e6, 4 * seqs * width),
        compiler_params=room(62),
        name="scale",
    )(tokens, gain, weight)


def split_kernel(nz, where, down, *refs):
    outs, sems = refs[:-1], refs[-1]
    nt = len(outs)
    chunk = outs[0].shape[1] // nz
    copies = []
    for s in range(nt):
        other = lax.rem(where[3] + s, nt)
        for i in range(nz):
            at = pl.multiple_of((i * nt + other) * chunk, chunk)
            copies.append(
                pltpu.make_async_copy(
                    down.at[:, pl.ds(at, chunk)],
                    outs[s].at[:, pl.ds(i * chunk, chunk)],
                    sems.at[s, i],
                )
            )
    run(copies)


def split(where, down, nz, nt):
    rows, cols = down.shape
    return pl.pallas_call(
        functools.partial(split_kernel, nz),
        out_shape=[shaped((rows, cols // nt), bf16)] * nt,
        in_specs=[SMEM, HBM],
        out_specs=[VMEM] * nt,
        scratch_shapes=[pltpu.SemaphoreType.DMA((nt, nz))],
        cost_estimate=cost(1e6, 4 * rows * cols),
        compiler_params=room(62),
        name="split",
    )(where, down)


def project_kernel(nx, nz, where, tok, *refs):
    own, other = refs[:nx], refs[nx : 2 * nx]
    outs = refs[2 * nx : 2 * nx + nz]
    weight = refs[-1]
    z, x, c = where[0], where[1], where[2]
    rows = own[0].shape[0]
    seqs = outs[0].shape[0]
    for i in range(nx):
        base = lax.rem(x - i + nx, nx) * (2 * rows)
        weight[pl.ds(pl.multiple_of(base + c * rows, rows), rows), :] = own[i][...]
        weight[pl.ds(pl.multiple_of(base + (1 - c) * rows, rows), rows), :] = other[i][...]
    left = jnp.concatenate(
        [tok[lax.rem(z + s, nz), :seqs].astype(f32) for s in range(nz)], axis=0
    ).astype(bf16)
    total = jnp.dot(left, weight[...], preferred_element_type=f32)
    for s in range(nz):
        outs[s][...] = total[s * seqs : (s + 1) * seqs].astype(bf16)


def project(where, tok, seqs, own, other):
    nz, _, depth = tok.shape
    nx, cols = len(own), own[0].shape[1]
    return pl.pallas_call(
        functools.partial(project_kernel, nx, nz),
        out_shape=[shaped((seqs, cols), bf16)] * nz,
        in_specs=[SMEM] + [VMEM] * (1 + 2 * nx),
        out_specs=[VMEM] * nz,
        scratch_shapes=[pltpu.VMEM((depth, cols), bf16)],
        cost_estimate=cost(2 * nz * seqs * depth * cols, 2 * depth * cols),
        compiler_params=room(10),
        name="project",
    )(where, tok, *own, *other)


def attend_kernel(step, count, *refs):
    arrived, refs = refs[:count], refs[count:]
    scale, shift_of, state_at, gain, out, state, sems = refs
    seqs, heads = state.shape[:2]
    copies = [
        pltpu.make_async_copy(
            state_at.at[pl.ds(i * step, step)], state.at[pl.ds(i * step, step)], sems.at[i]
        )
        for i in range(seqs // step)
    ]
    for copy in copies:
        copy.start()
    total = arrived[0][...].astype(f32)
    for ref in arrived[1:]:
        total = total + ref[...].astype(f32)
    total = total * scale[:, :1]
    rows = step
    keys = shift_of.shape[1]
    vals = out.shape[1]
    dim, width = keys // heads, vals // heads
    query = total[:, :keys] * dim ** (-0.5)
    key = total[:, keys : 2 * keys]
    pre = total[:, 2 * keys : 3 * keys]
    value = total[:, 3 * keys : 3 * keys + vals]
    rgate = total[:, 3 * keys + vals :]
    log_sig = jnp.minimum(pre, 0.0) - jnp.log1p(jnp.exp(-jnp.abs(pre)))
    faded = query * jnp.exp(log_sig / tau + shift_of[...])
    product = query * key
    silu = rgate * jax.nn.sigmoid(rgate)
    turned = [jnp.transpose(faded[:, h * dim : (h + 1) * dim]) for h in range(heads)]
    reads = [[] for _ in range(heads)]
    for i in range(seqs // rows):
        copies[i].wait()
        for s in range(i * rows, (i + 1) * rows):
            for h in range(heads):
                reads[h].append(
                    jnp.sum(turned[h][:, s : s + 1] * state[s, h], axis=0, keepdims=True)
                )
    for h in range(heads):
        at = slice(h * dim, (h + 1) * dim)
        cols = slice(h * width, (h + 1) * width)
        read = jnp.concatenate(reads[h], axis=0)
        read = read + jnp.sum(product[:, at], axis=-1, keepdims=True) * value[:, cols]
        meansq = jnp.mean(read * read, axis=-1, keepdims=True)
        out[:, cols] = (
            read
            * lax.rsqrt(meansq + eps)
            * gain[...].astype(f32).reshape(1, -1)[:, cols]
            * silu[:, cols]
        ).astype(bf16)


def attend(arrived, scale, decay_shift, state, head_gain):
    seqs, heads, _, width = state.shape
    step = 8
    vals = heads * width
    return pl.pallas_call(
        functools.partial(attend_kernel, step, len(arrived)),
        out_shape=shaped((seqs, vals), bf16),
        in_specs=[VMEM] * (len(arrived) + 2) + [HBM, VMEM],
        out_specs=VMEM,
        scratch_shapes=[
            pltpu.VMEM(state.shape, f32),
            pltpu.SemaphoreType.DMA((seqs // step,)),
        ],
        cost_estimate=cost(4 * state.size, 4 * state.size),
        compiler_params=room(52),
        name="attend",
    )(*arrived, scale, decay_shift, state, head_gain)


def mix_kernel(nx, where, gated, partner, *refs):
    blocks = refs[:nx]
    outs = refs[nx : 2 * nx]
    weight, sems = refs[-2:]
    x, t = where[1], where[3]
    copies = []
    for i in range(nx):
        copy = pltpu.make_async_copy(
            blocks[i], weight.at[lax.rem(x - i + nx, nx)], sems.at[i]
        )
        copy.start()
        copies.append(copy)
    rows = jnp.concatenate([gated[...], partner[...]], axis=0)
    for copy in copies:
        copy.wait()
    _, nz, cols, depth = weight.shape
    for s in range(nx):
        block = weight[lax.rem(t + s, nx)].reshape(nz * cols, depth)
        outs[s][...] = lax.dot_general(
            rows, block, (((1,), (1,)), ((), ())), preferred_element_type=f32
        ).astype(bf16)


def mix(where, gated, partner, blocks):
    nx = len(blocks)
    nz, rows, depth = blocks[0].shape
    cols = nz * rows
    seqs = 2 * gated.shape[0]
    return pl.pallas_call(
        functools.partial(mix_kernel, nx),
        out_shape=[shaped((seqs, cols), bf16)] * nx,
        in_specs=[SMEM, VMEM, VMEM] + [ANY] * nx,
        out_specs=[VMEM] * nx,
        scratch_shapes=[
            pltpu.VMEM((nx, nz, rows, depth), bf16),
            pltpu.SemaphoreType.DMA((nx,)),
        ],
        cost_estimate=cost(2 * seqs * cols * nx * depth, 2 * cols * nx * depth),
        compiler_params=room(8),
        name="mix",
    )(where, gated, partner, *blocks)


def put_rows(values, wide):
    chunks = values.shape[1] // 128
    for j in range(chunks):
        wide[pl.ds(j, values.shape[0], stride=chunks), :] = values[:, j * 128 : (j + 1) * 128]
    return wide[...].astype(bf16)


def dispatch_kernel(nz, nt, where, tokens, gain, sender, mine, other, out, stream, wide):
    c, t = where[2], where[3]
    chunk = stream.shape[1] // nz
    half = chunk // 2
    first, second = mine[...].astype(f32), other[...].astype(f32)
    first, second = jnp.where(c == 0, first, second), jnp.where(c == 0, second, first)
    for i in range(nz):
        own = tokens[:, pl.ds(pl.multiple_of((i * nt + t) * chunk, chunk), chunk)]
        at = slice(i * half, (i + 1) * half)
        mixed = jnp.concatenate([first[:, at], second[:, at]], axis=1)
        stream[:, i * chunk : (i + 1) * chunk] = own.astype(f32) + mixed
    rows = jnp.dot(
        sender[...], (stream[...] * gain[t]).astype(bf16), preferred_element_type=f32
    )
    out[...] = put_rows(rows, wide)


def dispatch(where, tokens, gain, sender, mine, other, nz, nt):
    slots, seqs = sender.shape
    part = 2 * mine.shape[1]
    wide = slots * part // 128
    return pl.pallas_call(
        functools.partial(dispatch_kernel, nz, nt),
        out_shape=[shaped((wide, 128), bf16), shaped((seqs, part), f32)],
        in_specs=[SMEM] + [VMEM] * 5,
        out_specs=[VMEM] * 2,
        scratch_shapes=[pltpu.VMEM((wide, 128), f32)],
        cost_estimate=cost(2 * slots * seqs * part, 6 * slots * part),
        compiler_params=room(6),
        name="dispatch",
    )(where, tokens, gain, sender, mine, other)


def take_rows(rows, wide, slots):
    wide[...] = rows[...].astype(f32)
    chunks = wide.shape[0] // slots
    return jnp.concatenate(
        [wide[pl.ds(j, slots, stride=chunks), :] for j in range(chunks)], axis=1
    )


def pick_kernel(nt, where, w_gate, w_lin, *refs):
    outs, sems = refs[:nt], refs[nt]
    units = w_gate.shape[-1]
    copies = []
    for s in range(nt):
        at = lax.rem(where[3] - s + nt, nt)
        for k, ref in enumerate((w_gate, w_lin)):
            copy = pltpu.make_async_copy(
                ref.at[:, at], outs[s].at[:, :, pl.ds(k * units, units)], sems.at[s, k]
            )
            copy.start()
            copies.append(copy)
    for copy in copies:
        copy.wait()


def pick(where, w_gate, w_lin):
    nz, nt, chunk, units = w_gate.shape
    return pl.pallas_call(
        functools.partial(pick_kernel, nt),
        out_shape=[shaped((nz, chunk, 2 * units), bf16)] * nt,
        in_specs=[SMEM, HBM, HBM],
        out_specs=[VMEM] * nt,
        scratch_shapes=[pltpu.SemaphoreType.DMA((nt, 2))],
        cost_estimate=cost(1e6, 4 * w_gate.size),
        compiler_params=room(8),
        name="pick",
    )(where, w_gate, w_lin)


def expert_kernel(step, nt, first, last, where, inverse, weight, piece, *refs):
    if not first:
        before, refs = refs[:2], refs[2:]
    outs, wide = refs[:-1], refs[-1]
    slots = outs[0].shape[0]
    rows = take_rows(piece, wide, slots)
    plain = rows * inverse[lax.rem(where[3] - step + nt, nt)]
    plain = plain * plain
    part = rows.shape[1]
    sumsq = plain[:, :128]
    for j in range(1, part // 128):
        sumsq = sumsq + plain[:, j * 128 : (j + 1) * 128]
    total = jnp.dot(
        rows.astype(bf16), weight[...].reshape(part, -1), preferred_element_type=f32
    )
    if not first:
        total = total + before[0][...]
        sumsq = sumsq + before[1][...]
    if not last:
        outs[0][...] = total
        outs[1][...] = sumsq
        return
    units = outs[0].shape[1]
    meansq = jnp.sum(sumsq, axis=-1, keepdims=True) / (nt * part)
    total = total * lax.rsqrt(meansq + eps)
    gate = jnp.minimum(total[:, :units], limit)
    lin = jnp.clip(total[:, units:], -limit, limit)
    outs[0][...] = (gate * jax.nn.sigmoid(glu_alpha * gate) * (lin + 1.0)).astype(bf16)


def expert(where, inverse, weight, step, nt, piece, slots, before=(), last=False):
    units = weight.shape[-1]
    out_shape = (
        shaped((slots, units // 2), bf16)
        if last
        else [shaped((slots, units), f32), shaped((slots, 128), f32)]
    )
    return pl.pallas_call(
        functools.partial(expert_kernel, step, nt, not before, last),
        out_shape=out_shape,
        in_specs=[SMEM] + [VMEM] * (3 + len(before)),
        out_specs=VMEM if last else [VMEM] * 2,
        scratch_shapes=[pltpu.VMEM(piece.shape, f32)],
        cost_estimate=cost(2 * slots * weight.size, 2 * weight.size),
        compiler_params=room(8),
        name="expert",
    )(where, inverse, weight, piece, *before)


def fetch_kernel(*refs):
    count = len(refs) - 2
    out, sems = refs[count:]
    rows = refs[0].shape[0]
    run(
        [
            pltpu.make_async_copy(ref, out.at[pl.ds(i * rows, rows)], sems.at[i])
            for i, ref in enumerate(refs[:count])
        ]
    )


def fetch(arrays):
    rows, cols = arrays[0].shape
    return pl.pallas_call(
        fetch_kernel,
        out_shape=shaped((rows * len(arrays), cols), bf16),
        in_specs=[HBM] * len(arrays),
        out_specs=VMEM,
        scratch_shapes=[pltpu.SemaphoreType.DMA((len(arrays),))],
        cost_estimate=cost(1e6, 4 * len(arrays) * rows * cols),
        compiler_params=room(4),
        name="fetch",
    )(*arrays)


def down_kernel(nt, *refs):
    acts = refs[:nt]
    weight, out, wide = refs[nt:]
    act = jnp.concatenate([ref[...] for ref in acts], axis=1)
    total = jnp.dot(act, weight[...], preferred_element_type=f32)
    out[...] = put_rows(total, wide)


def down_sum(acts, weight):
    nt = len(acts)
    slots, units = acts[0].shape
    part = weight.shape[1]
    wide = slots * part // 128
    return pl.pallas_call(
        functools.partial(down_kernel, nt),
        out_shape=shaped((wide, 128), bf16),
        scratch_shapes=[pltpu.VMEM((wide, 128), f32)],
        cost_estimate=cost(2 * nt * slots * units * part, 2 * nt * units * part),
        compiler_params=room(8),
        name="down",
    )(*acts, weight)


def combine_kernel(rows, weights, stream, out, wide):
    wide[...] = rows[...].astype(f32)
    seqs, part = out.shape
    chunks = part // 128
    slots = wide.shape[0] // chunks
    for j in range(chunks):
        values = wide[pl.ds(j, slots, stride=chunks), :].astype(bf16)
        sums = jnp.dot(weights[...], values, preferred_element_type=f32)
        routed = sums[:seqs] + sums[seqs : 2 * seqs] + sums[2 * seqs :]
        at = slice(j * 128, (j + 1) * 128)
        out[:, at] = (stream[:, at] + routed).astype(bf16)


def combine(rows, weights, stream):
    return pl.pallas_call(
        combine_kernel,
        out_shape=shaped(stream.shape, bf16),
        scratch_shapes=[pltpu.VMEM(rows.shape, f32)],
        cost_estimate=cost(2 * weights.size * stream.shape[1], 2 * rows.size),
        compiler_params=room(4),
        name="combine",
    )(rows, weights, stream)


def finish_kernel(nz, where, *refs):
    pieces, out = refs[:-1], refs[-1]
    nt = len(pieces)
    chunk = pieces[0].shape[1] // nz
    for s in range(nt):
        other = lax.rem(where[3] - s + nt, nt)
        for i in range(nz):
            at = pl.multiple_of((i * nt + other) * chunk, chunk)
            out[:, pl.ds(at, chunk)] = pieces[s][:, i * chunk : (i + 1) * chunk]


def finish(where, pieces, nz):
    seqs, part = pieces[0].shape
    return pl.pallas_call(
        functools.partial(finish_kernel, nz),
        out_shape=shaped((seqs, part * len(pieces)), bf16),
        in_specs=[SMEM] + [VMEM] * len(pieces),
        out_specs=VMEM,
        cost_estimate=cost(1e6, 4 * seqs * part * len(pieces)),
        compiler_params=room(2),
        name="finish",
    )(where, *pieces)


def to_bf16(value):
    return lax.reduce_precision(value, 8, 7)


def routing(expert_ids, route_weight, n_ep):
    seq_dev, top = expert_ids.shape
    flat_ids = expert_ids.reshape(-1)
    onehot = (flat_ids[:, None] == jnp.arange(n_ep, dtype=jnp.int32)[None, :]).astype(jnp.int32)
    rank = jnp.sum((jnp.cumsum(onehot, axis=0) - onehot) * onehot, axis=1)
    slot_of = (flat_ids * CAP + rank).reshape(seq_dev, top)
    slots = n_ep * CAP
    hits = jnp.arange(slots, dtype=jnp.int32)[None, None, :] == slot_of[:, :, None]
    sender = jnp.sum(hits.astype(f32), axis=1).T.astype(bf16)
    weights = jnp.sum(jnp.where(hits, route_weight[:, :, None], 0.0), axis=1)
    return sender, weights


def three_parts(weights):
    high = to_bf16(weights)
    middle = to_bf16(weights - high)
    low = weights - high - middle
    return jnp.concatenate([high, middle, low], axis=0).astype(bf16)


def on_device(
    tokens,
    norm_gain,
    w_query,
    w_key,
    w_value,
    w_rgate,
    w_decay,
    decay_shift,
    state,
    head_gain,
    w_out,
    ffn_gain,
    w_gate,
    w_lin,
    w_down,
    expert_ids,
    route_weight,
):
    width = tokens.shape[1]
    nz, nx, nt = lax.axis_size(Z), lax.axis_size(X), lax.axis_size(T)
    n_ep = lax.axis_size(EP)
    slots = n_ep * CAP
    part = width // nt
    chunk = part // nz
    where = jnp.stack([lax.axis_index(a) for a in (Z, X, C, T)]).astype(jnp.int32)

    packed = pack((w_query, w_key, w_decay, w_value, w_rgate))
    own = [packed] + [shift(packed, X, i) for i in range(1, nx)]
    other = [shift(packed, C, 1)]
    other += [shift(w, C, 1) for w in own[1:]]

    seqs = tokens.shape[0]
    payload, first_scale = scale(tokens, norm_gain, w_out.T, nz)
    moved = lax.all_to_all(payload, Z, 0, 0, tiled=True)
    out_z = moved[:, seqs:]
    blocks = [out_z] + [None] * (nx - 1)
    for i in range(1, nx):
        blocks[i] = shift(out_z, X, i)

    downs = split(where, w_down[0], nz, nt)
    downs = [downs[0]] + [shift(downs[s], T, s) for s in range(1, nt)]

    sender, weights = routing(expert_ids, route_weight, n_ep)
    gain_of = ffn_gain.astype(f32).reshape(nz, nt, chunk)
    gain_of = jnp.moveaxis(gain_of, 1, 0).reshape(nt, 1, part)
    inverse = 1.0 / gain_of
    weights = three_parts(weights)

    parts = project(where, moved, seqs, own, other)
    arrived = [parts[0]]
    for i in order_of(nz):
        arrived.append(shift(parts[i], Z, i))
    gated = attend(arrived, first_scale, decay_shift, state, head_gain)
    partner = shift(gated, C, 1)
    mixed = mix(where, gated, partner, blocks)
    mixed = spread(mixed)
    mine = functools.reduce(jnp.add, [m[:seqs].astype(f32) for m in mixed]).astype(bf16)
    theirs = functools.reduce(jnp.add, [m[seqs:].astype(f32) for m in mixed]).astype(bf16)
    other_half = shift(theirs, C, 1)
    outbound, stream = dispatch(
        where, tokens, gain_of, sender, mine, other_half, nz, nt
    )
    rows = lax.all_to_all(
        outbound.reshape(n_ep, -1, 128), EP, 0, 0, tiled=True
    ).reshape(-1, 128)
    pieces = [rows] + [shift(rows, T, s) for s in range(1, nt)]
    gates = w_gate.reshape(nz, nt, chunk, -1)
    lins = w_lin.reshape(nz, nt, chunk, -1)
    picked = pick(where, gates, lins)
    fetched = fetch(downs)
    before = ()
    steps = [0] + order_of(nt)[1:] + [nt // 2]
    for s in steps:
        before = expert(
            where, inverse, picked[s], s, nt, pieces[s], slots, before, s == steps[-1]
        )
    act = before
    acts = spread([act] * nt)
    done = down_sum(acts, fetched)
    returned = lax.all_to_all(
        done.reshape(n_ep, -1, 128), EP, 0, 0, tiled=True
    ).reshape(-1, 128)
    result = combine(returned, weights, stream)
    results = spread([result] * nt)
    return finish(where, results, nz)


def solution(mesh):
    sizes = dict(mesh.shape)
    torus = Mesh(
        mesh.devices.reshape(sizes.get("z", 8), sizes.get("x", 4), 2, sizes["tp"]),
        (Z, X, C, T),
    )
    return jax.shard_map(
        on_device,
        mesh=torus,
        in_specs=(
            P(EP, None),
            P(),
            P(EP, T),
            P(EP, T),
            P(EP, T),
            P(EP, T),
            P(EP, T),
            P(EP, T),
            P(EP, T, None, None),
            P(T),
            P(T, EP),
            P(),
            P(EP, None, T),
            P(EP, None, T),
            P(EP, T, None),
            P(EP, None),
            P(EP, None),
        ),
        out_specs=P(EP, None),
        check_vma=False,
    )
```
